32 devices in a mesh: sp: 8 (over z, y), tp: 4 (over x, core).
Axes of the slice: x: 2, y: 2, z: 4, core: 2. Of those that a mesh axis runs over, the one named last changes fastest.
Arguments:
- latent: bfloat16 [2048, 2048], P('sp'), may hold values from -6 to 6
- context: bfloat16 [512, 2048], P('sp'), may hold values from -6 to 6
- condition: float32 [2048], P('sp'), may hold values from -6 to 6
- ctx_condition: float32 [2048], P('sp'), may hold values from -6 to 6
- shift_weight: bfloat16 [2048, 2048], P('sp', 'tp'), may hold values from -0.125 to 0.125
- scale_weight: bfloat16 [2048, 2048], P('sp', 'tp'), may hold values from -0.125 to 0.125
- gate_weight: bfloat16 [2048, 2048], P('sp', 'tp'), may hold values from -0.125 to 0.125
- norm_gain: float32 [2048], replicated, may hold values from 0.1 to 1.9
- query_weight: bfloat16 [2048, 1024], P(None, 'tp'), may hold values from -0.125 to 0.125
- key_weight: bfloat16 [2048, 1024], P(None, 'tp'), may hold values from -0.125 to 0.125
- value_weight: bfloat16 [2048, 1024], P(None, 'tp'), may hold values from -0.125 to 0.125
- query_gain: float32 [64], replicated, may hold values from 0.6 to 6.5
- key_gain: float32 [64], replicated, may hold values from 0.6 to 6.5
- offset_bias: float32 [16, 15, 31], P('tp'), may hold values from 1 to 3
- out_weight: bfloat16 [1024, 2048], P('tp'), may hold values from -0.75 to 0.75
Outputs:
- mixed_rows: bfloat16 [2048, 2048], P('sp')
The draws below stay inside these ranges and needn't reach their ends.
All inputs are finite; a program needn't handle non-finite values.
Results may differ from the reference program's by a relative error of at most 0.01405.
The reference program's roundings to bfloat16 on the way count: a program that leaves them out, or rounds other values in their place, can miss the bound.
Values may be sent and summed in bfloat16 or wider, within the bound.
No kernel may reach another device: no remote copies, remote signals or barrier semaphores. Data moves between devices by JAX's collectives and lax.ppermute only.
A program may use at most 64 MiB of HBM per device.

```python
import jax
import jax.numpy as jnp
from jax import lax

D = 2048
HEADS = 16
HEAD_DIM = 64
GRID_W = 64
WIN_ROWS = 8
WIN_COLS = 16
CTX = 512
TOKENS = 2048
ATT_W = 1024
N_TP = 4


def gain_draw(base_key):
    return jax.random.uniform(base_key, (HEAD_DIM,), jnp.float32, 0.6, 2.0)


def draw_query_gain(key, part):
    return gain_draw(jax.random.fold_in(key, 11))


def draw_key_gain(key, part):
    return gain_draw(jax.random.fold_in(key, 23))


def level_of(stream_key, dims, cuts, smallest, largest):
    gain = 1.0
    for dim, shards_of in cuts:
        heights = jax.random.uniform(jax.random.fold_in(jax.random.fold_in(stream_key, 6), dim), (shards_of,), jnp.float32, smallest / len(cuts), largest / len(cuts))
        gain = gain * jnp.repeat(jnp.exp(heights), dims[dim] // shards_of).reshape((-1,) + (1,) * (len(dims) - 1 - dim))
    return gain


def gaussian(rng, extent, width, most, cuts=(), kind=jnp.bfloat16):
    values = width * jax.random.normal(rng, extent, jnp.float32)
    if cuts:
        values = values * level_of(rng, extent, cuts, -0.22, 0.18)
    return jnp.clip(values, -most, most).astype(kind)


def setup_inputs(seed: int = 0) -> dict:
    streams_of = jax.random.split(jax.random.key(seed), 16)
    latent = gaussian(streams_of[0], (TOKENS, D), 1.0, 6.0, ((0, 8),))
    context = gaussian(streams_of[1], (CTX, D), 1.0, 6.0, ((0, 8),))
    condition = gaussian(streams_of[2], (D,), 1.0, 6.0, ((0, 8),), jnp.float32)
    ctx_condition = gaussian(streams_of[3], (D,), 1.0, 6.0, ((0, 8),), jnp.float32)
    shift_weight = gaussian(streams_of[4], (D, D), D ** -0.5, 0.125, ((0, 8), (1, 4)))
    scale_weight = gaussian(streams_of[5], (D, D), D ** -0.5, 0.125, ((0, 8), (1, 4)))
    gate_weight = gaussian(streams_of[6], (D, D), D ** -0.5, 0.125, ((0, 8), (1, 4)))
    norm_gain = jnp.clip(1.0 + 0.18 * jax.random.normal(streams_of[7], (D,), jnp.float32), 0.1, 1.9)
    query_weight = gaussian(streams_of[8], (D, ATT_W), D ** -0.5, 0.125, ((1, 4),))
    key_weight = gaussian(streams_of[9], (D, ATT_W), D ** -0.5, 0.125, ((1, 4),))
    value_weight = gaussian(streams_of[10], (D, ATT_W), D ** -0.5, 0.125, ((1, 4),))
    query_gain = draw_query_gain(jax.random.fold_in(streams_of[15], 71), 0)
    key_gain = draw_key_gain(jax.random.fold_in(streams_of[15], 71), 0)
    offset_bias = jnp.clip(1.0 + 2.0 * jax.random.uniform(streams_of[13], (HEADS, 2 * WIN_ROWS - 1, 2 * WIN_COLS - 1), jnp.float32) ** level_of(streams_of[13], (HEADS, 2 * WIN_ROWS - 1, 2 * WIN_COLS - 1), ((0, 4),), -0.2, 0.2), 1.0, 3.0)
    out_weight = gaussian(streams_of[14], (ATT_W, D), (ATT_W // 16) ** -0.5, 0.75, ((0, 4),))
    return dict(latent=latent, context=context, condition=condition, ctx_condition=ctx_condition, shift_weight=shift_weight, scale_weight=scale_weight, gate_weight=gate_weight, norm_gain=norm_gain, query_weight=query_weight, key_weight=key_weight, value_weight=value_weight, query_gain=query_gain, key_gain=key_gain, offset_bias=offset_bias, out_weight=out_weight)


EPS = 1e-06

def modulate(rows_in, norm_gain, shift_vec, scale_vec):
    values = rows_in.astype(jnp.float32)
    normed = values * lax.rsqrt(lax.optimization_barrier(jnp.mean(values * values, axis=-1, keepdims=True)) + EPS)
    return (normed * norm_gain * (1.0 + scale_vec) + shift_vec).astype(jnp.bfloat16)

def head_norm(projected, head_gain):
    row_count = projected.shape[0]
    split_heads = projected.reshape(row_count, -1, head_gain.shape[0])
    normed = split_heads * lax.rsqrt(lax.optimization_barrier(jnp.mean(split_heads * split_heads, axis=-1, keepdims=True)) + EPS)
    return (normed * head_gain).astype(jnp.bfloat16).reshape(row_count, -1)

def per_head(matrix, row_count):
    return matrix.reshape(row_count, HEADS, HEAD_DIM).transpose(1, 0, 2)

def reference(latent, context, condition, ctx_condition, shift_weight, scale_weight, gate_weight, norm_gain, query_weight, key_weight, value_weight, query_gain, key_gain, offset_bias, out_weight):
    activations = jax.nn.silu(jnp.stack([condition, ctx_condition])).astype(jnp.bfloat16)
    shift_vec = jnp.dot(activations, shift_weight, preferred_element_type=jnp.float32)
    scale_vec = jnp.dot(activations, scale_weight, preferred_element_type=jnp.float32)
    gate_vec = jnp.dot(activations[:1], gate_weight, preferred_element_type=jnp.float32)
    hidden = modulate(latent, norm_gain, shift_vec[0], scale_vec[0])
    ctx_hidden = modulate(context, norm_gain, shift_vec[1], scale_vec[1])
    queries = head_norm(jnp.dot(hidden, query_weight, preferred_element_type=jnp.float32), query_gain)
    keys_lat = head_norm(jnp.dot(hidden, key_weight, preferred_element_type=jnp.float32), key_gain)
    values_lat = jnp.dot(hidden, value_weight, preferred_element_type=jnp.float32).astype(jnp.bfloat16)
    ctx_keys = head_norm(jnp.dot(ctx_hidden, key_weight, preferred_element_type=jnp.float32), key_gain)
    ctx_values = jnp.dot(ctx_hidden, value_weight, preferred_element_type=jnp.float32).astype(jnp.bfloat16)
    grid_rows = TOKENS // GRID_W
    score_scale = HEAD_DIM ** (-0.5)
    row_ids = jnp.arange(grid_rows, dtype=jnp.int32)
    band_start = jnp.clip(row_ids - WIN_ROWS // 2, 0, grid_rows - WIN_ROWS)
    band_rows = band_start[:, None] + jnp.arange(WIN_ROWS, dtype=jnp.int32)[None, :]
    row_steps = band_rows - row_ids[:, None] + WIN_ROWS - 1
    column_ids = jnp.arange(GRID_W, dtype=jnp.int32)
    col_start = jnp.clip(column_ids - WIN_COLS // 2, 0, GRID_W - WIN_COLS)
    col_open = (column_ids[None, :] >= col_start[:, None]) & (column_ids[None, :] < col_start[:, None] + WIN_COLS)
    col_steps = jnp.clip(column_ids[None, :] - column_ids[:, None], 1 - WIN_COLS, WIN_COLS - 1) + WIN_COLS - 1

    def one_head(operands):
        q_head, k_head, v_head, kc_head, vc_head, table = operands
        q_grid = q_head.reshape(grid_rows, GRID_W, HEAD_DIM).astype(jnp.float32)
        k_grid = k_head.reshape(grid_rows, GRID_W, HEAD_DIM).astype(jnp.float32)
        v_grid = v_head.reshape(grid_rows, GRID_W, HEAD_DIM).astype(jnp.float32)
        k_band = k_grid[band_rows]
        v_band = v_grid[band_rows]
        offsets = table[row_steps[:, None, :, None], col_steps[None, :, None, :]]
        local_scores = jnp.einsum('rqd,rjkd->rqjk', q_grid, k_band) * score_scale + offsets
        local_scores = jnp.where(col_open[None, :, None, :], local_scores, -jnp.inf)
        ctx_scores = jnp.einsum('rqd,nd->rqn', q_grid, kc_head.astype(jnp.float32)) * score_scale
        row_max = jnp.maximum(lax.optimization_barrier(jnp.max(local_scores, axis=(2, 3))), lax.optimization_barrier(jnp.max(ctx_scores, axis=2)))
        local_exp = jnp.exp(local_scores - row_max[..., None, None])
        ctx_exp = jnp.exp(ctx_scores - row_max[..., None])
        denominator = lax.optimization_barrier(jnp.sum(local_exp, axis=(2, 3))) + lax.optimization_barrier(jnp.sum(ctx_exp, axis=2))
        local_weights = (local_exp / denominator[..., None, None]).astype(jnp.bfloat16)
        ctx_weights = (ctx_exp / denominator[..., None]).astype(jnp.bfloat16)
        result = jnp.einsum('rqjk,rjkd->rqd', local_weights.astype(jnp.float32), v_band) + jnp.einsum('rqn,nd->rqd', ctx_weights.astype(jnp.float32), vc_head.astype(jnp.float32))
        return result.astype(jnp.bfloat16)
    attended = lax.map(one_head, (per_head(queries, TOKENS), per_head(keys_lat, TOKENS), per_head(values_lat, TOKENS), per_head(ctx_keys, CTX), per_head(ctx_values, CTX), offset_bias))
    attended = attended.transpose(1, 2, 0, 3).reshape(TOKENS, ATT_W)
    group_cols = ATT_W // N_TP
    branch = jnp.zeros((TOKENS, D), jnp.float32)
    for group in range(N_TP):
        partial_value = jnp.dot(attended[:, group * group_cols:(group + 1) * group_cols], out_weight[group * group_cols:(group + 1) * group_cols], preferred_element_type=jnp.float32)
        rounded = lax.optimization_barrier(partial_value.astype(jnp.bfloat16))
        branch = branch + rounded.astype(jnp.float32)
    return (latent.astype(jnp.float32) + gate_vec[0] * branch).astype(jnp.bfloat16)
```

```python
import functools

import jax
import jax.numpy as jnp
from jax import lax
from jax.experimental import pallas as pl
from jax.experimental.pallas import tpu as pltpu
from jax.sharding import PartitionSpec as P

HEAD_DIM = 64
GRID_W = 64
WIN_ROWS = 8
WIN_COLS = 16
LANES = 128
EPS = 1e-06
MASKED = -1e30

F32 = jnp.float32
BF16 = jnp.bfloat16


def vmem(count):
    return [pl.BlockSpec(memory_space=pltpu.VMEM) for _ in range(count)]


def params(mib):
    return pltpu.CompilerParams(vmem_limit_bytes=mib << 20)


def swap(x, axis, code):
    count = lax.axis_size(axis)
    return lax.ppermute(x, axis, [(i, i ^ code) for i in range(count)])


def bits_of(axis):
    count = lax.axis_size(axis)
    return [1 << b for b in range(count.bit_length() - 1)]


def bt_dot(a, b):
    return lax.dot_general(a, b, (((1,), (1,)), ((), ())), preferred_element_type=F32)


def partials_body(cond_ref, ctx_cond_ref, shift_ref, scale_ref, gate_ref, out_ref):
    rows = jnp.concatenate([cond_ref[...], ctx_cond_ref[...]], axis=0)
    act = (rows / (1.0 + jnp.exp(-rows))).astype(BF16)
    out_ref[0:2, :] = jnp.dot(act, shift_ref[...], preferred_element_type=F32)
    out_ref[2:4, :] = jnp.dot(act, scale_ref[...], preferred_element_type=F32)
    out_ref[4:6, :] = jnp.dot(act, gate_ref[...], preferred_element_type=F32)
    out_ref[6:8, :] = jnp.zeros((2, out_ref.shape[1]), F32)


def table_body(bias_ref, out_ref):
    heads, pairs = out_ref.shape[:2]
    q = lax.broadcasted_iota(jnp.int32, (GRID_W, 2 * GRID_W), 0)
    lane = lax.broadcasted_iota(jnp.int32, (GRID_W, 2 * GRID_W), 1)
    k = lane & (GRID_W - 1)
    start = jnp.clip(q - WIN_COLS // 2, 0, GRID_W - WIN_COLS)
    is_open = (k >= start) & (k < start + WIN_COLS)
    low = lane < GRID_W
    width = 2 * GRID_W
    for h in range(heads):
        rolled = []
        for a in range(pairs + 1):
            row = jnp.broadcast_to(bias_ref[h, a : a + 1, :], (GRID_W, width))
            rolled.append(row)
        for a in range(pairs):
            first = pltpu.roll(rolled[a], (1 - WIN_COLS) % width, 1, stride=1, stride_axis=0)
            second = pltpu.roll(
                rolled[a + 1], (1 - WIN_COLS + GRID_W) % width, 1, stride=1, stride_axis=0
            )
            out_ref[h, a] = jnp.where(is_open, jnp.where(low, first, second), MASKED)


def project_body(codes, tp_ref, lat_ref, ctx_ref, *refs):
    count = len(codes)
    blocks = refs[:count]
    gain_ref, wq_ref, wk_ref, wv_ref, qg_ref, kg_ref = refs[count : count + 6]
    q_ref, kv_ref, ckv_ref, gate_ref, vec_ref, hid_ref = refs[count + 6 :]
    width = blocks[0].shape[1]
    me = tp_ref[0]
    for code, block in zip(codes, blocks):
        at = pl.multiple_of((me ^ code) * width, width)
        vec_ref[:, pl.ds(at, width)] = block[...]
    gate_ref[...] = vec_ref[4:5, :]
    lat_count = lat_ref.shape[0]
    ctx_count = ctx_ref.shape[0]
    gain = gain_ref[...]
    for src, base, count_rows, row in ((lat_ref, 0, lat_count, 0), (ctx_ref, lat_count, ctx_count, 1)):
        mult = gain * (1.0 + vec_ref[2 + row : 3 + row, :])
        shift = vec_ref[row : row + 1, :]
        step = min(32, count_rows)
        for at in range(0, count_rows, step):
            values = src[at : at + step, :].astype(F32)
            mean = jnp.mean(values * values, axis=-1, keepdims=True)
            hid = values * lax.rsqrt(mean + EPS) * mult + shift
            hid_ref[base + at : base + at + step, :] = hid.astype(BF16)
    cols = wq_ref.shape[1]
    r = lax.broadcasted_iota(jnp.int32, (cols, cols), 0) // HEAD_DIM
    c = lax.broadcasted_iota(jnp.int32, (cols, cols), 1) // HEAD_DIM
    same = jnp.where(r == c, 1.0 / HEAD_DIM, 0.0).astype(BF16)

    def head_norm(x, head_gain):
        square = x * x
        high = square.astype(BF16)
        rest = (square - high.astype(F32)).astype(BF16)
        mean = jnp.dot(high, same, preferred_element_type=F32) + jnp.dot(
            rest, same, preferred_element_type=F32
        )
        return (x * lax.rsqrt(mean + EPS) * head_gain).astype(BF16)

    hidden = hid_ref[...]
    keys = head_norm(jnp.dot(hidden, wk_ref[...], preferred_element_type=F32), kg_ref[...])
    kv_ref[:, :cols] = keys[:lat_count]
    ckv_ref[:, :cols] = keys[lat_count:]
    values = jnp.dot(hidden, wv_ref[...], preferred_element_type=F32).astype(BF16)
    kv_ref[:, cols:] = values[:lat_count]
    ckv_ref[:, cols:] = values[lat_count:]
    queries = head_norm(
        jnp.dot(hidden[:lat_count], wq_ref[...], preferred_element_type=F32), qg_ref[...]
    )
    q_ref[...] = (queries.astype(F32) * HEAD_DIM ** (-0.5)).astype(BF16)


def attend_body(heads, n_ctx, starts_ref, q_ref, up_ref, own_ref, down_ref, *refs):
    ctx_refs = refs[:n_ctx]
    table_ref, out_ref = refs[n_ctx:]
    cols = q_ref.shape[1]
    tokens = q_ref.shape[0]
    rows = tokens // GRID_W
    parts = (up_ref, own_ref, down_ref)
    halo = WIN_ROWS // 2
    lane_head = lax.broadcasted_iota(jnp.int32, (1, cols), 1) // HEAD_DIM
    lane = lax.broadcasted_iota(jnp.int32, (1, 2 * GRID_W), 1)
    q_all = q_ref[...]
    keys = [p[:, :cols] for p in parts] + [p[:, :cols] for p in ctx_refs]
    values = [p[:, cols:] for p in parts] + [p[:, cols:] for p in ctx_refs]
    n_rows = rows + 2 * halo
    opens = []
    for i in range(rows):
        start = starts_ref[i]
        opens.append(
            [
                jnp.where(
                    (lane // GRID_W + 2 * p >= start)
                    & (lane // GRID_W + 2 * p < start + WIN_ROWS),
                    0.0,
                    MASKED,
                )
                for p in range(n_rows // 2)
            ]
        )
    total = jnp.zeros((tokens, cols), F32)
    for h in range(heads):
        mine = lane_head == h
        q_h = jnp.where(mine, q_all, jnp.zeros_like(q_all))
        scores = [bt_dot(q_h, k) for k in keys]
        biased = []
        for part in range(3):
            per_part = parts[part].shape[0] // GRID_W
            base = (0, halo, halo + rows)[part]
            lines = []
            for i in range(rows):
                line = []
                for p in range(per_part // 2):
                    j = base + 2 * p
                    a = j - i + WIN_ROWS - 1 - halo
                    piece = scores[part][
                        i * GRID_W : (i + 1) * GRID_W, 2 * p * GRID_W : (2 * p + 2) * GRID_W
                    ]
                    line.append(piece + (table_ref[h, a] + opens[i][j // 2]))
                lines.append(jnp.concatenate(line, axis=1))
            biased.append(jnp.concatenate(lines, axis=0))
        scores = biased + scores[3:]
        top = functools.reduce(jnp.maximum, [jnp.max(s, axis=1, keepdims=True) for s in scores])
        powers = [jnp.exp(s - top) for s in scores]
        denom = functools.reduce(jnp.add, [jnp.sum(e, axis=1, keepdims=True) for e in powers])
        inv = 1.0 / denom
        acc = functools.reduce(
            jnp.add,
            [
                jnp.dot((e * inv).astype(BF16), v, preferred_element_type=F32)
                for e, v in zip(powers, values)
            ],
        )
        total = jnp.where(mine, acc, total)
    out_ref[...] = total.astype(BF16)


def output_body(count, lat_ref, gate_ref, *refs):
    att = refs[:count]
    weights = refs[count : 2 * count]
    out_ref = refs[2 * count]
    branch = None
    for a, w in zip(att, weights):
        part = jnp.dot(a[...], w[...], preferred_element_type=F32).astype(BF16).astype(F32)
        branch = part if branch is None else branch + part
    out_ref[...] = (lat_ref[...].astype(F32) + gate_ref[...] * branch).astype(BF16)


def gather_pieces(x, axis, codes):
    pieces = [x]
    for code in codes:
        if len(pieces) > 2:
            pieces = [jnp.concatenate(pieces, axis=0)]
        pieces = pieces + [swap(p, axis, code) for p in pieces]
    return pieces


def gather_tp(x, codes):
    held = [(0, x)]
    for code in codes:
        held = held + [(had ^ code, swap(p, "tp", code)) for had, p in held]
    return held


def per_device(
    latent,
    context,
    condition,
    ctx_condition,
    shift_weight,
    scale_weight,
    gate_weight,
    norm_gain,
    query_weight,
    key_weight,
    value_weight,
    query_gain,
    key_gain,
    offset_bias,
    out_weight,
):
    sp_bits = bits_of("sp")
    tp_bits = bits_of("tp")[::-1]
    tokens, width = latent.shape
    cols = query_weight.shape[1]
    heads = cols // HEAD_DIM
    rows = tokens // GRID_W
    halo = WIN_ROWS // 2
    block_cols = shift_weight.shape[1]

    ctx_two = jnp.concatenate([context, swap(context, "sp", sp_bits[0])], axis=0)
    part = pl.pallas_call(
        partials_body,
        out_shape=jax.ShapeDtypeStruct((8, block_cols), F32),
        in_specs=vmem(5),
        out_specs=vmem(1)[0],
        compiler_params=params(16),
        name="partials",
    )(condition[None], ctx_condition[None], shift_weight, scale_weight, gate_weight)
    for code in sp_bits[1:] + sp_bits[:1]:
        part = part + swap(part, "sp", code)
    vec_blocks = gather_tp(part, tp_bits)
    ow_blocks = gather_tp(out_weight, tp_bits)

    padded_bias = jnp.pad(offset_bias, ((0, 0), (0, 0), (0, LANES - offset_bias.shape[2])))
    tables = pl.pallas_call(
        table_body,
        out_shape=jax.ShapeDtypeStruct((heads, 2 * WIN_ROWS - 2, GRID_W, 2 * GRID_W), F32),
        in_specs=vmem(1),
        out_specs=vmem(1)[0],
        compiler_params=params(16),
        name="tables",
    )(padded_bias)

    codes = tuple(code for code, _ in vec_blocks)
    ctx_count = ctx_two.shape[0]
    tp_index = lax.axis_index("tp").astype(jnp.int32).reshape(1)
    smem = pl.BlockSpec(memory_space=pltpu.SMEM)
    queries, kv, ctx_kv, gate = pl.pallas_call(
        functools.partial(project_body, codes),
        out_shape=(
            jax.ShapeDtypeStruct((tokens, cols), BF16),
            jax.ShapeDtypeStruct((tokens, 2 * cols), BF16),
            jax.ShapeDtypeStruct((ctx_count, 2 * cols), BF16),
            jax.ShapeDtypeStruct((1, width), F32),
        ),
        in_specs=[smem] + vmem(2 + len(codes) + 6),
        out_specs=vmem(4),
        scratch_shapes=[
            pltpu.VMEM((8, width), F32),
            pltpu.VMEM((tokens + ctx_count, width), BF16),
        ],
        compiler_params=params(24),
        name="project",
    )(
        tp_index,
        latent,
        ctx_two,
        *[block for _, block in vec_blocks],
        norm_gain[None],
        query_weight,
        key_weight,
        value_weight,
        jnp.tile(query_gain, heads)[None],
        jnp.tile(key_gain, heads)[None],
    )

    sp_count = lax.axis_size("sp")
    up = lax.ppermute(kv, "sp", [(i, i + 1) for i in range(sp_count - 1)])
    down = lax.ppermute(kv, "sp", [(i + 1, i) for i in range(sp_count - 1)])
    ctx_pieces = gather_pieces(ctx_kv, "sp", sp_bits[1:][::-1])

    first_row = lax.axis_index("sp") * rows
    total_rows = rows * sp_count
    row_ids = first_row + jnp.arange(rows, dtype=jnp.int32)
    starts = jnp.clip(row_ids - halo, 0, total_rows - WIN_ROWS) - first_row + halo
    n_ctx = len(ctx_pieces)
    attended = pl.pallas_call(
        functools.partial(attend_body, heads, n_ctx),
        out_shape=jax.ShapeDtypeStruct((tokens, cols), BF16),
        in_specs=[smem] + vmem(4 + n_ctx + 1),
        out_specs=vmem(1)[0],
        compiler_params=params(32),
        name="attend",
    )(starts.astype(jnp.int32), queries, up, kv, down, *ctx_pieces, tables)

    att_blocks = gather_tp(attended, tp_bits)
    count = len(att_blocks)
    tile = min(512, width)
    whole = pl.BlockSpec((tokens, cols), lambda n: (0, 0))
    return pl.pallas_call(
        functools.partial(output_body, count),
        grid=(width // tile,),
        out_shape=jax.ShapeDtypeStruct((tokens, width), BF16),
        in_specs=[
            pl.BlockSpec((tokens, tile), lambda n: (0, n)),
            pl.BlockSpec((1, tile), lambda n: (0, n)),
        ]
        + [whole] * count
        + [pl.BlockSpec((cols, tile), lambda n: (0, n))] * count,
        out_specs=pl.BlockSpec((tokens, tile), lambda n: (0, n)),
        compiler_params=params(24),
        name="output",
    )(latent, gate, *[a for _, a in att_blocks], *[w for _, w in ow_blocks])


def solution(mesh):
    in_specs = (
        P("sp", None),
        P("sp", None),
        P("sp"),
        P("sp"),
        P("sp", "tp"),
        P("sp", "tp"),
        P("sp", "tp"),
        P(),
        P(None, "tp"),
        P(None, "tp"),
        P(None, "tp"),
        P(),
        P(),
        P("tp", None, None),
        P("tp", None),
    )
    out_specs = P("sp", None)
    return jax.shard_map(
        per_device, mesh=mesh, in_specs=in_specs, out_specs=out_specs, check_vma=False
    )
```

```python
import functools

import jax
import jax.numpy as jnp
from jax import lax
from jax.experimental import pallas as pl
from jax.experimental.pallas import tpu as pltpu
from jax.sharding import PartitionSpec as P


HEAD_DIM = 64
GRID_W = 64
WIN_ROWS = 8
WIN_COLS = 16
LANES = 128
EPS = 1e-06
MASKED = -1e30

F32 = jnp.float32
BF16 = jnp.bfloat16


def vmem(count):
    return [pl.BlockSpec(memory_space=pltpu.VMEM) for _ in range(count)]


def params(mib):
    return pltpu.CompilerParams(vmem_limit_bytes=mib << 20)


def swap(x, axis, code):
    return lax.ppermute(x, axis, [(i, i ^ code) for i in range(lax.axis_size(axis))])


def call(*args, **kwargs):
    def run(*operands):
        return pl.pallas_call(*args, **kwargs)(*operands)

    return run


def in_hbm(x):
    return pltpu.with_memory_space_constraint(x, pltpu.HBM)


def raw(count):
    return [pl.BlockSpec(memory_space=pltpu.HBM) for _ in range(count)]


def bits_of(axis):
    count = lax.axis_size(axis)
    return [1 << b for b in range(count.bit_length() - 1)]


def bt_dot(a, b):
    return lax.dot_general(a, b, (((1,), (1,)), ((), ())), preferred_element_type=F32)


def partials_body(
    cond_ref, ctx_cond_ref, shift_ref, scale_ref, gate_ref, out_ref, rows_ref, *scratch
):
    weights, sems = scratch[:3], scratch[3]
    copies = [
        pltpu.make_async_copy(cond_ref, rows_ref.at[0:1], sems.at[3]),
        pltpu.make_async_copy(ctx_cond_ref, rows_ref.at[1:2], sems.at[4]),
    ] + [
        pltpu.make_async_copy(src, dst, sems.at[n])
        for n, (src, dst) in enumerate(zip((shift_ref, scale_ref, gate_ref), weights))
    ]
    for copy in copies:
        copy.start()
    copies[0].wait()
    copies[1].wait()
    rows = rows_ref[...]
    act = (rows / (1.0 + jnp.exp(-rows))).astype(BF16)
    for n in range(3):
        copies[2 + n].wait()
        out_ref[2 * n : 2 * n + 2, :] = jnp.dot(
            act, weights[n][...], preferred_element_type=F32
        )
    out_ref[6:8, :] = jnp.zeros((2, out_ref.shape[1]), F32)


def table_body(bias_ref, out_ref):
    heads, pairs = out_ref.shape[:2]
    q = lax.broadcasted_iota(jnp.int32, (GRID_W, 2 * GRID_W), 0)
    lane = lax.broadcasted_iota(jnp.int32, (GRID_W, 2 * GRID_W), 1)
    k = lane & (GRID_W - 1)
    start = jnp.clip(q - WIN_COLS // 2, 0, GRID_W - WIN_COLS)
    is_open = (k >= start) & (k < start + WIN_COLS)
    low = lane < GRID_W
    width = 2 * GRID_W
    for h in range(heads):
        rolled = []
        for a in range(pairs + 1):
            row = jnp.broadcast_to(bias_ref[h, a : a + 1, :], (GRID_W, width))
            rolled.append(row)
        for a in range(pairs):
            first = pltpu.roll(rolled[a], (1 - WIN_COLS) % width, 1, stride=1, stride_axis=0)
            second = pltpu.roll(
                rolled[a + 1], (1 - WIN_COLS + GRID_W) % width, 1, stride=1, stride_axis=0
            )
            out_ref[h, a] = jnp.where(is_open, jnp.where(low, first, second), MASKED)


def head_norm(x, gain_row):
    cols = x.shape[1]
    r = lax.broadcasted_iota(jnp.int32, (cols, cols), 0) // HEAD_DIM
    c = lax.broadcasted_iota(jnp.int32, (cols, cols), 1) // HEAD_DIM
    same = jnp.where(r == c, 1.0 / HEAD_DIM, 0.0).astype(BF16)
    head_gain = jnp.concatenate([gain_row[...]] * (cols // HEAD_DIM), axis=1)
    square = x * x
    high = square.astype(BF16)
    rest = (square - high.astype(F32)).astype(BF16)
    mean = jnp.dot(high, same, preferred_element_type=F32) + jnp.dot(
        rest, same, preferred_element_type=F32
    )
    return x * lax.rsqrt(mean + EPS) * head_gain


def project_body(codes, n_ctx, lat_ref, *refs):
    count = len(codes)
    ctx_refs, refs = refs[:n_ctx], refs[n_ctx:]
    blocks, refs = refs[:count], refs[count:]
    gain_ref, kg_ref, wk, wv = refs[:4]
    kv_ref, ckv_ref, lat_hid_ref, gate_ref = refs[4:8]
    vec_ref, hid_ref = refs[8:]
    width = blocks[0].shape[1]
    me = lax.axis_index("tp")
    for code, block in zip(codes, blocks):
        at = pl.multiple_of((me ^ code) * width, width)
        vec_ref[:, pl.ds(at, width)] = block[...]
    gate_ref[...] = vec_ref[4:5, :]
    lat_count = lat_ref.shape[0]
    gain = gain_ref[...]

    def modulated(values, row):
        mult = gain * (1.0 + vec_ref[2 + row : 3 + row, :])
        shift = vec_ref[row : row + 1, :]
        mean = jnp.mean(values * values, axis=-1, keepdims=True)
        return (values * lax.rsqrt(mean + EPS) * mult + shift).astype(BF16)

    step = 32
    for at in range(0, lat_count, step):
        hid_ref[at : at + step, :] = modulated(lat_ref[at : at + step, :].astype(F32), 0)
    if ctx_refs[0].shape[0] % step:
        both = jnp.concatenate([c[...].astype(F32) for c in ctx_refs], axis=0)
        hid_ref[lat_count:, :] = modulated(both, 1)
    else:
        base = lat_count
        for c in ctx_refs:
            for at in range(0, c.shape[0], step):
                hid_ref[base : base + step, :] = modulated(c[at : at + step, :].astype(F32), 1)
                base += step
    cols = wk.shape[1]
    hidden = hid_ref[...]
    keys = head_norm(jnp.dot(hidden, wk[...], preferred_element_type=F32), kg_ref).astype(BF16)
    kv_ref[:, :cols] = keys[:lat_count]
    ckv_ref[:, :cols] = keys[lat_count:]
    values = jnp.dot(hidden, wv[...], preferred_element_type=F32).astype(BF16)
    kv_ref[:, cols:] = values[:lat_count]
    ckv_ref[:, cols:] = values[lat_count:]
    lat_hid_ref[...] = hidden[:lat_count]


def query_body(hid_ref, wq_ref, qg_ref, q_ref):
    queries = head_norm(
        jnp.dot(hid_ref[...], wq_ref[...], preferred_element_type=F32), qg_ref
    ).astype(BF16)
    q_ref[...] = (queries.astype(F32) * HEAD_DIM ** (-0.5)).astype(BF16)


OWN, NEAR, OTHER = range(3)


def attend_body(heads, lat_kinds, n_ctx, has_prev, is_last, q_ref, *refs):
    n_lat = len(lat_kinds)
    lat_refs, refs = refs[:n_lat], refs[n_lat:]
    ctx_refs, refs = refs[:n_ctx], refs[n_ctx:]
    if n_lat:
        table_ref, refs = refs[0], refs[1:]
    if has_prev:
        prev, refs = refs[:3], refs[3:]
    tokens, cols = q_ref.shape
    rows = tokens // GRID_W
    halo = WIN_ROWS // 2
    lane_head = lax.broadcasted_iota(jnp.int32, (1, cols), 1) // HEAD_DIM
    lane_row = lax.broadcasted_iota(jnp.int32, (1, 2 * GRID_W), 1) // GRID_W
    q_all = q_ref[...]
    parts = list(lat_refs) + list(ctx_refs)
    keys = [p[:, :cols] for p in parts]
    values = [p[:, cols:] for p in parts]
    sp_index = lax.axis_index("sp")
    first_row = sp_index * rows
    total_rows = rows * lax.axis_size("sp")
    starts = [
        jnp.clip(first_row + i - halo, 0, total_rows - WIN_ROWS) - first_row + halo
        for i in range(rows)
    ]
    is_odd = lax.rem(sp_index, 2)
    base_of = {
        OWN: halo,
        NEAR: (1 - is_odd) * (halo + rows),
        OTHER: is_odd * (halo + rows),
    }
    bases = [base_of[kind] for kind in lat_kinds]
    opens = {}
    for n in range(n_lat):
        for i in range(rows):
            for p in range(lat_refs[n].shape[0] // (2 * GRID_W)):
                row = lane_row + (bases[n] + 2 * p)
                start = starts[i]
                opens[n, i, p] = jnp.where(
                    (row >= start) & (row < start + WIN_ROWS), 0.0, MASKED
                )
    tops = jnp.zeros((tokens, cols), F32)
    sums = jnp.zeros((tokens, cols), F32)
    total = jnp.zeros((tokens, cols), F32)
    for h in range(heads):
        mine = lane_head == h
        q_h = jnp.where(mine, q_all, jnp.zeros_like(q_all))
        scores = [bt_dot(q_h, k) for k in keys]
        for n in range(n_lat):
            lines = []
            for i in range(rows):
                line = []
                for p in range(lat_refs[n].shape[0] // (2 * GRID_W)):
                    at = bases[n] + 2 * p - i + WIN_ROWS - 1 - halo
                    piece = scores[n][
                        i * GRID_W : (i + 1) * GRID_W, 2 * p * GRID_W : (2 * p + 2) * GRID_W
                    ]
                    line.append(piece + (table_ref[h, at] + opens[n, i, p]))
                lines.append(jnp.concatenate(line, axis=1))
            scores[n] = jnp.concatenate(lines, axis=0)
        top = functools.reduce(jnp.maximum, [jnp.max(s, axis=1, keepdims=True) for s in scores])
        powers = [jnp.exp(s - top) for s in scores]
        denom = functools.reduce(jnp.add, [jnp.sum(e, axis=1, keepdims=True) for e in powers])
        acc = functools.reduce(
            jnp.add,
            [
                jnp.dot(e.astype(BF16), v, preferred_element_type=F32)
                for e, v in zip(powers, values)
            ],
        )
        tops = jnp.where(mine, top, tops)
        sums = jnp.where(mine, denom, sums)
        total = jnp.where(mine, acc, total)
    if has_prev:
        before = prev[0][...]
        both = jnp.maximum(before, tops)
        old = jnp.exp(before - both)
        new = jnp.exp(tops - both)
        tops = both
        sums = prev[1][...] * old + sums * new
        total = prev[2][...] * old + total * new
    if is_last:
        refs[0][...] = (total / sums).astype(BF16)
    else:
        for ref, value in zip(refs, (tops, sums, total)):
            ref[...] = value


def first_body(count, *refs):
    att, weights, sum_ref = refs[:count], refs[count : 2 * count], refs[2 * count]
    branch = None
    for a, w in zip(att, weights):
        part = jnp.dot(a[...], w[...], preferred_element_type=F32).astype(BF16).astype(F32)
        branch = part if branch is None else branch + part
    sum_ref[...] = branch


def output_body(count, lat_ref, gate_ref, sum_ref, *refs):
    att = refs[:count]
    weights = refs[count : 2 * count]
    out_ref = refs[2 * count]
    branch = sum_ref[...]
    for a, w in zip(att, weights):
        branch = branch + jnp.dot(a[...], w[...], preferred_element_type=F32).astype(
            BF16
        ).astype(F32)
    out_ref[...] = (lat_ref[...].astype(F32) + gate_ref[...] * branch).astype(BF16)


def gather_pieces(x, axis, codes):
    pieces = [x]
    for code in codes:
        if len(pieces) > 2:
            pieces = [jnp.concatenate(pieces, axis=0)]
        pieces = pieces + [swap(p, axis, code) for p in pieces]
    return pieces


def gather_tp(x, codes):
    held = [(0, x)]
    for code in codes:
        held = held + [(had ^ code, swap(p, "tp", code)) for had, p in held]
    return held


def per_device(
    latent,
    context,
    condition,
    ctx_condition,
    shift_weight,
    scale_weight,
    gate_weight,
    norm_gain,
    query_weight,
    key_weight,
    value_weight,
    query_gain,
    key_gain,
    offset_bias,
    out_weight,
):
    sp_bits = bits_of("sp")
    tp_bits = bits_of("tp")[::-1]
    tokens, width = latent.shape
    cols = query_weight.shape[1]
    heads = cols // HEAD_DIM
    block_cols = shift_weight.shape[1]

    raw_codes = [code for code in RAW_CODES if code in sp_bits]
    ctx_parts = gather_pieces(context, "sp", raw_codes)
    part = call(
        partials_body,
        out_shape=jax.ShapeDtypeStruct((8, block_cols), F32),
        in_specs=raw(5),
        out_specs=vmem(1)[0],
        scratch_shapes=[pltpu.VMEM((2, condition.shape[0]), F32)]
        + [pltpu.VMEM(shift_weight.shape, BF16)] * 3
        + [pltpu.SemaphoreType.DMA((5,))],
        compiler_params=params(16),
        cost_estimate=pl.CostEstimate(flops=1 << 37, bytes_accessed=1 << 20, transcendentals=0),
    )(*[in_hbm(x) for x in (condition[None], ctx_condition[None], shift_weight, scale_weight, gate_weight)])
    for code in sp_bits[1:] + sp_bits[:1]:
        part = part + swap(part, "sp", code)
    vec_blocks = gather_tp(part, tp_bits)
    ow_blocks = gather_tp(out_weight, tp_bits)

    padded_bias = jnp.pad(offset_bias, ((0, 0), (0, 0), (0, LANES - offset_bias.shape[2])))
    tables = call(
        table_body,
        out_shape=jax.ShapeDtypeStruct((heads, 2 * WIN_ROWS - 2, GRID_W, 2 * GRID_W), F32),
        in_specs=vmem(1),
        out_specs=vmem(1)[0],
        compiler_params=params(16),
    )(padded_bias)

    codes = tuple(code for code, _ in vec_blocks)
    ctx_count = len(ctx_parts) * ctx_parts[0].shape[0]
    kv, ctx_kv, hidden, gate = call(
        functools.partial(project_body, codes, len(ctx_parts)),
        out_shape=(
            jax.ShapeDtypeStruct((tokens, 2 * cols), BF16),
            jax.ShapeDtypeStruct((ctx_count, 2 * cols), BF16),
            jax.ShapeDtypeStruct((tokens, width), BF16),
            jax.ShapeDtypeStruct((1, width), F32),
        ),
        in_specs=vmem(1 + len(ctx_parts) + len(codes) + 4),
        out_specs=vmem(4),
        scratch_shapes=[
            pltpu.VMEM((8, width), F32),
            pltpu.VMEM((tokens + ctx_count, width), BF16),
        ],
        compiler_params=params(20),
        cost_estimate=pl.CostEstimate(flops=1 << 37, bytes_accessed=1 << 20, transcendentals=0),
    )(
        latent,
        *ctx_parts,
        *[block for _, block in vec_blocks],
        norm_gain[None],
        key_gain[None],
        key_weight,
        value_weight,
    )
    queries = call(
        query_body,
        out_shape=jax.ShapeDtypeStruct((tokens, cols), BF16),
        in_specs=vmem(3),
        out_specs=vmem(1)[0],
        compiler_params=params(8),
    )(hidden, query_weight, query_gain[None])

    sp_count = lax.axis_size("sp")
    other_pairs = [(i, i + 1) for i in range(1, sp_count - 1, 2)]
    other_pairs += [(j, i) for i, j in other_pairs]
    near_kv = swap(kv, "sp", 1)
    other_kv = lax.ppermute(kv, "sp", other_pairs)
    ctx_pieces = gather_pieces(
        ctx_kv, "sp", [code for code in sp_bits[::-1] if code not in raw_codes]
    )

    def attend(lat, lat_kinds, ctx, prev, is_last):
        shape = (tokens, cols)
        one = jax.ShapeDtypeStruct(shape, BF16)
        three = (jax.ShapeDtypeStruct(shape, F32),) * 3
        operands = [queries, *lat, *ctx] + ([tables] if lat else []) + list(prev)
        return call(
            functools.partial(
                attend_body, heads, lat_kinds, len(ctx), bool(prev), is_last
            ),
            out_shape=one if is_last else three,
            in_specs=vmem(len(operands)),
            out_specs=vmem(1)[0] if is_last else tuple(vmem(3)),
            compiler_params=params(24),
            cost_estimate=pl.CostEstimate(
                flops=1 << 37, bytes_accessed=1 << 20, transcendentals=0
            ),
        )(*operands)

    state = attend([kv], (OWN,), ctx_pieces[:1], (), False)
    attended = attend([near_kv, other_kv], (NEAR, OTHER), ctx_pieces[1:], state, True)

    att_blocks = gather_tp(attended, tp_bits)
    near = [n for n, (code, _) in enumerate(att_blocks) if code < 2]
    far = [n for n in range(len(att_blocks)) if n not in near]
    tile = min(512, width)
    att_spec = pl.BlockSpec((tokens, cols), lambda n: (0, 0))
    weight_spec = pl.BlockSpec((cols, tile), lambda n: (0, n))
    wide_spec = pl.BlockSpec((tokens, tile), lambda n: (0, n))
    partial_sum = call(
        functools.partial(first_body, len(near)),
        grid=(width // tile,),
        out_shape=jax.ShapeDtypeStruct((tokens, width), F32),
        in_specs=[att_spec] * len(near) + [weight_spec] * len(near),
        out_specs=wide_spec,
        compiler_params=params(24),
    )(*[att_blocks[n][1] for n in near], *[ow_blocks[n][1] for n in near])
    return call(
        functools.partial(output_body, len(far)),
        grid=(width // tile,),
        out_shape=jax.ShapeDtypeStruct((tokens, width), BF16),
        in_specs=[wide_spec, pl.BlockSpec((1, tile), lambda n: (0, n)), wide_spec]
        + [att_spec] * len(far)
        + [weight_spec] * len(far),
        out_specs=wide_spec,
        compiler_params=params(24),
    )(
        latent,
        gate,
        partial_sum,
        *[att_blocks[n][1] for n in far],
        *[ow_blocks[n][1] for n in far],
    )


RAW_CODES = (1,)


def solution(mesh):
    in_specs = (
        P("sp", None),
        P("sp", None),
        P("sp"),
        P("sp"),
        P("sp", "tp"),
        P("sp", "tp"),
        P("sp", "tp"),
        P(),
        P(None, "tp"),
        P(None, "tp"),
        P(None, "tp"),
        P(),
        P(),
        P("tp", None, None),
        P("tp", None),
    )
    out_specs = P("sp", None)
    return jax.shard_map(
        per_device, mesh=mesh, in_specs=in_specs, out_specs=out_specs, check_vma=False
    )
```

```python
import functools

import jax
import jax.numpy as jnp
from jax import lax
from jax.experimental import pallas as pl
from jax.experimental.pallas import tpu as pltpu
from jax.sharding import PartitionSpec as P


HEAD_DIM = 64
GRID_W = 64
WIN_ROWS = 8
WIN_COLS = 16
LANES = 128
EPS = 1e-06
MASKED = -1e30

F32 = jnp.float32
BF16 = jnp.bfloat16


def vmem(count):
    return [pl.BlockSpec(memory_space=pltpu.VMEM) for _ in range(count)]


def params(mib):
    return pltpu.CompilerParams(vmem_limit_bytes=mib << 20)


def swap(x, axis, code):
    return lax.ppermute(x, axis, [(i, i ^ code) for i in range(lax.axis_size(axis))])


def call(*args, **kwargs):
    def run(*operands):
        return pl.pallas_call(*args, **kwargs)(*operands)

    return run


def in_hbm(x):
    return pltpu.with_memory_space_constraint(x, pltpu.HBM)


def raw(count):
    return [pl.BlockSpec(memory_space=pltpu.HBM) for _ in range(count)]


def bits_of(axis):
    count = lax.axis_size(axis)
    return [1 << b for b in range(count.bit_length() - 1)]


def bt_dot(a, b):
    return lax.dot_general(a, b, (((1,), (1,)), ((), ())), preferred_element_type=F32)


def partials_body(
    cond_ref, ctx_cond_ref, shift_ref, scale_ref, gate_ref, out_ref, rows_ref, *scratch
):
    weights, sems = scratch[:3], scratch[3]
    copies = [
        pltpu.make_async_copy(cond_ref, rows_ref.at[0:1], sems.at[3]),
        pltpu.make_async_copy(ctx_cond_ref, rows_ref.at[1:2], sems.at[4]),
    ] + [
        pltpu.make_async_copy(src, dst, sems.at[n])
        for n, (src, dst) in enumerate(zip((shift_ref, scale_ref, gate_ref), weights))
    ]
    for copy in copies:
        copy.start()
    copies[0].wait()
    copies[1].wait()
    rows = rows_ref[...]
    act = (rows / (1.0 + jnp.exp(-rows))).astype(BF16)
    for n in range(3):
        copies[2 + n].wait()
        out_ref[2 * n : 2 * n + 2, :] = jnp.dot(
            act, weights[n][...], preferred_element_type=F32
        )
    out_ref[6:8, :] = jnp.zeros((2, out_ref.shape[1]), F32)


def table_body(bias_ref, out_ref):
    heads, pairs = out_ref.shape[:2]
    q = lax.broadcasted_iota(jnp.int32, (GRID_W, 2 * GRID_W), 0)
    lane = lax.broadcasted_iota(jnp.int32, (GRID_W, 2 * GRID_W), 1)
    k = lane & (GRID_W - 1)
    start = jnp.clip(q - WIN_COLS // 2, 0, GRID_W - WIN_COLS)
    is_open = (k >= start) & (k < start + WIN_COLS)
    low = lane < GRID_W
    width = 2 * GRID_W
    for h in range(heads):
        rolled = []
        for a in range(pairs + 1):
            row = jnp.broadcast_to(bias_ref[h, a : a + 1, :], (GRID_W, width))
            rolled.append(row)
        for a in range(pairs):
            first = pltpu.roll(rolled[a], (1 - WIN_COLS) % width, 1, stride=1, stride_axis=0)
            second = pltpu.roll(
                rolled[a + 1], (1 - WIN_COLS + GRID_W) % width, 1, stride=1, stride_axis=0
            )
            out_ref[h, a] = jnp.where(is_open, jnp.where(low, first, second), MASKED)


def head_norm(x, gain_row):
    cols = x.shape[1]
    r = lax.broadcasted_iota(jnp.int32, (cols, cols), 0) // HEAD_DIM
    c = lax.broadcasted_iota(jnp.int32, (cols, cols), 1) // HEAD_DIM
    same = jnp.where(r == c, 1.0 / HEAD_DIM, 0.0).astype(BF16)
    head_gain = jnp.concatenate([gain_row[...]] * (cols // HEAD_DIM), axis=1)
    square = x * x
    high = square.astype(BF16)
    rest = (square - high.astype(F32)).astype(BF16)
    mean = jnp.dot(high, same, preferred_element_type=F32) + jnp.dot(
        rest, same, preferred_element_type=F32
    )
    return x * lax.rsqrt(mean + EPS) * head_gain


def project_body(codes, n_ctx, lat_ref, *refs):
    ctx_refs, refs = refs[:n_ctx], refs[n_ctx:]
    part_ref, beside_ref, refs = refs[0], refs[1], refs[2:]
    gain_ref, kg_ref, wk, wv = refs[:4]
    kv_ref, ckv_ref, lat_hid_ref, gate_ref = refs[4:8]
    vec_ref, hid_ref = refs[8:]
    width = part_ref.shape[1]
    me = lax.axis_index("tp")
    for n, code in enumerate(codes):
        for ref, flip in ((part_ref, 0), (beside_ref, 1)):
            at = pl.multiple_of((me ^ code ^ flip) * width, width)
            vec_ref[:, pl.ds(at, width)] = ref[8 * n : 8 * n + 8, :]
    gate_ref[...] = vec_ref[4:5, :]
    lat_count = lat_ref.shape[0]
    gain = gain_ref[...]

    def modulated(values, row):
        mult = gain * (1.0 + vec_ref[2 + row : 3 + row, :])
        shift = vec_ref[row : row + 1, :]
        mean = jnp.mean(values * values, axis=-1, keepdims=True)
        return (values * lax.rsqrt(mean + EPS) * mult + shift).astype(BF16)

    step = 32
    for at in range(0, lat_count, step):
        hid_ref[at : at + step, :] = modulated(lat_ref[at : at + step, :].astype(F32), 0)
    if ctx_refs[0].shape[0] % step:
        both = jnp.concatenate([c[...].astype(F32) for c in ctx_refs], axis=0)
        hid_ref[lat_count:, :] = modulated(both, 1)
    else:
        base = lat_count
        for c in ctx_refs:
            for at in range(0, c.shape[0], step):
                hid_ref[base : base + step, :] = modulated(c[at : at + step, :].astype(F32), 1)
                base += step
    cols = wk.shape[1]
    hidden = hid_ref[...]
    keys = head_norm(jnp.dot(hidden, wk[...], preferred_element_type=F32), kg_ref).astype(BF16)
    kv_ref[:, :cols] = keys[:lat_count]
    ckv_ref[:, :cols] = keys[lat_count:]
    values = jnp.dot(hidden, wv[...], preferred_element_type=F32).astype(BF16)
    kv_ref[:, cols:] = values[:lat_count]
    ckv_ref[:, cols:] = values[lat_count:]
    lat_hid_ref[...] = hidden[:lat_count]


def query_body(hid_ref, wq_ref, qg_ref, q_ref):
    queries = head_norm(
        jnp.dot(hid_ref[...], wq_ref[...], preferred_element_type=F32), qg_ref
    ).astype(BF16)
    q_ref[...] = (queries.astype(F32) * HEAD_DIM ** (-0.5)).astype(BF16)


OWN, NEAR, OTHER = range(3)


def attend_body(heads, lat_kinds, n_ctx, has_prev, is_last, q_ref, *refs):
    n_lat = len(lat_kinds)
    lat_refs, refs = refs[:n_lat], refs[n_lat:]
    ctx_refs, refs = refs[:n_ctx], refs[n_ctx:]
    if n_lat:
        table_ref, refs = refs[0], refs[1:]
    if has_prev:
        prev, refs = refs[:3], refs[3:]
    tokens, cols = q_ref.shape
    rows = tokens // GRID_W
    halo = WIN_ROWS // 2
    lane_head = lax.broadcasted_iota(jnp.int32, (1, cols), 1) // HEAD_DIM
    lane_row = lax.broadcasted_iota(jnp.int32, (1, 2 * GRID_W), 1) // GRID_W
    q_all = q_ref[...]
    parts = list(lat_refs) + list(ctx_refs)
    keys = [p[:, :cols] for p in parts]
    values = [p[:, cols:] for p in parts]
    sp_index = lax.axis_index("sp")
    first_row = sp_index * rows
    total_rows = rows * lax.axis_size("sp")
    starts = [
        jnp.clip(first_row + i - halo, 0, total_rows - WIN_ROWS) - first_row + halo
        for i in range(rows)
    ]
    is_odd = lax.rem(sp_index, 2)
    base_of = {
        OWN: halo,
        NEAR: (1 - is_odd) * (halo + rows),
        OTHER: is_odd * (halo + rows),
    }
    bases = [base_of[kind] for kind in lat_kinds]
    opens = {}
    for n in range(n_lat):
        for i in range(rows):
            for p in range(lat_refs[n].shape[0] // (2 * GRID_W)):
                row = lane_row + (bases[n] + 2 * p)
                start = starts[i]
                opens[n, i, p] = jnp.where(
                    (row >= start) & (row < start + WIN_ROWS), 0.0, MASKED
                )
    tops = jnp.zeros((tokens, cols), F32)
    sums = jnp.zeros((tokens, cols), F32)
    total = jnp.zeros((tokens, cols), F32)
    for h in range(heads):
        mine = lane_head == h
        q_h = jnp.where(mine, q_all, jnp.zeros_like(q_all))
        scores = [bt_dot(q_h, k) for k in keys]
        for n in range(n_lat):
            lines = []
            for i in range(rows):
                line = []
                for p in range(lat_refs[n].shape[0] // (2 * GRID_W)):
                    at = bases[n] + 2 * p - i + WIN_ROWS - 1 - halo
                    piece = scores[n][
                        i * GRID_W : (i + 1) * GRID_W, 2 * p * GRID_W : (2 * p + 2) * GRID_W
                    ]
                    line.append(piece + (table_ref[h, at] + opens[n, i, p]))
                lines.append(jnp.concatenate(line, axis=1))
            scores[n] = jnp.concatenate(lines, axis=0)
        top = functools.reduce(jnp.maximum, [jnp.max(s, axis=1, keepdims=True) for s in scores])
        powers = [jnp.exp(s - top) for s in scores]
        denom = functools.reduce(jnp.add, [jnp.sum(e, axis=1, keepdims=True) for e in powers])
        acc = functools.reduce(
            jnp.add,
            [
                jnp.dot(e.astype(BF16), v, preferred_element_type=F32)
                for e, v in zip(powers, values)
            ],
        )
        tops = jnp.where(mine, top, tops)
        sums = jnp.where(mine, denom, sums)
        total = jnp.where(mine, acc, total)
    if has_prev:
        before = prev[0][...]
        both = jnp.maximum(before, tops)
        old = jnp.exp(before - both)
        new = jnp.exp(tops - both)
        tops = both
        sums = prev[1][...] * old + sums * new
        total = prev[2][...] * old + total * new
    if is_last:
        refs[0][...] = (total / sums).astype(BF16)
    else:
        for ref, value in zip(refs, (tops, sums, total)):
            ref[...] = value


def stash_body(*refs):
    count = len(refs) // 2
    sems = refs[-1]
    copies = [
        pltpu.make_async_copy(src, dst, sems.at[n])
        for n, (src, dst) in enumerate(zip(refs[:count], refs[count : 2 * count]))
    ]
    for copy in copies:
        copy.start()
    for copy in copies:
        copy.wait()


def first_body(count, *refs):
    att, weights, sum_ref = refs[:count], refs[count : 2 * count], refs[2 * count]
    branch = None
    for a, w in zip(att, weights):
        part = jnp.dot(a[...], w[...], preferred_element_type=F32).astype(BF16).astype(F32)
        branch = part if branch is None else branch + part
    sum_ref[...] = branch


def output_body(count, lat_ref, gate_ref, sum_ref, *refs):
    att = refs[:count]
    weights = refs[count : 2 * count]
    out_ref = refs[2 * count]
    branch = sum_ref[...]
    for a, w in zip(att, weights):
        branch = branch + jnp.dot(a[...], w[...], preferred_element_type=F32).astype(
            BF16
        ).astype(F32)
    out_ref[...] = (lat_ref[...].astype(F32) + gate_ref[...] * branch).astype(BF16)


def gather_pieces(x, axis, codes):
    pieces = [x]
    for code in codes:
        if len(pieces) > 2:
            pieces = [jnp.concatenate(pieces, axis=0)]
        pieces = pieces + [swap(p, axis, code) for p in pieces]
    return pieces


def gather_tp(x, codes):
    held = [(0, x)]
    for code in codes:
        held = held + [(had ^ code, swap(p, "tp", code)) for had, p in held]
    return held


def per_device(
    latent,
    context,
    condition,
    ctx_condition,
    shift_weight,
    scale_weight,
    gate_weight,
    norm_gain,
    query_weight,
    key_weight,
    value_weight,
    query_gain,
    key_gain,
    offset_bias,
    out_weight,
):
    sp_bits = bits_of("sp")
    tp_bits = bits_of("tp")[::-1]
    tokens, width = latent.shape
    cols = query_weight.shape[1]
    heads = cols // HEAD_DIM
    block_cols = shift_weight.shape[1]

    raw_codes = [code for code in RAW_CODES if code in sp_bits]
    ctx_parts = gather_pieces(context, "sp", raw_codes)
    part = call(
        partials_body,
        out_shape=jax.ShapeDtypeStruct((8, block_cols), F32),
        in_specs=raw(5),
        out_specs=vmem(1)[0],
        scratch_shapes=[pltpu.VMEM((2, condition.shape[0]), F32)]
        + [pltpu.VMEM(shift_weight.shape, BF16)] * 3
        + [pltpu.SemaphoreType.DMA((5,))],
        compiler_params=params(16),
        cost_estimate=pl.CostEstimate(flops=1 << 37, bytes_accessed=1 << 20, transcendentals=0),
    )(*[in_hbm(x) for x in (condition[None], ctx_condition[None], shift_weight, scale_weight, gate_weight)])
    codes = [0]
    for code in tp_bits:
        if code > 1:
            part = jnp.concatenate([part, swap(part, "tp", code)], axis=0)
            codes = codes + [had ^ code for had in codes]
    for code in sp_bits[1:] + sp_bits[:1]:
        part = part + swap(part, "sp", code)
    beside = swap(part, "tp", 1)
    ow_blocks = gather_tp(out_weight, tp_bits)

    padded_bias = jnp.pad(offset_bias, ((0, 0), (0, 0), (0, LANES - offset_bias.shape[2])))
    tables = call(
        table_body,
        out_shape=jax.ShapeDtypeStruct((heads, 2 * WIN_ROWS - 2, GRID_W, 2 * GRID_W), F32),
        in_specs=vmem(1),
        out_specs=vmem(1)[0],
        compiler_params=params(16),
    )(padded_bias)

    ctx_count = len(ctx_parts) * ctx_parts[0].shape[0]
    kv, ctx_kv, hidden, gate = call(
        functools.partial(project_body, tuple(codes), len(ctx_parts)),
        out_shape=(
            jax.ShapeDtypeStruct((tokens, 2 * cols), BF16),
            jax.ShapeDtypeStruct((ctx_count, 2 * cols), BF16),
            jax.ShapeDtypeStruct((tokens, width), BF16),
            jax.ShapeDtypeStruct((1, width), F32),
        ),
        in_specs=vmem(1 + len(ctx_parts) + 2 + 4),
        out_specs=vmem(4),
        scratch_shapes=[
            pltpu.VMEM((8, width), F32),
            pltpu.VMEM((tokens + ctx_count, width), BF16),
        ],
        compiler_params=params(20),
        cost_estimate=pl.CostEstimate(flops=1 << 37, bytes_accessed=1 << 20, transcendentals=0),
    )(
        latent,
        *ctx_parts,
        part,
        beside,
        norm_gain[None],
        key_gain[None],
        key_weight,
        value_weight,
    )
    queries = call(
        query_body,
        out_shape=jax.ShapeDtypeStruct((tokens, cols), BF16),
        in_specs=vmem(3),
        out_specs=vmem(1)[0],
        compiler_params=params(8),
    )(hidden, query_weight, query_gain[None])

    sp_count = lax.axis_size("sp")
    other_pairs = [(i, i + 1) for i in range(1, sp_count - 1, 2)]
    other_pairs += [(j, i) for i, j in other_pairs]
    near_kv = swap(kv, "sp", 1)
    other_kv = lax.ppermute(kv, "sp", other_pairs)
    ctx_pieces = gather_pieces(
        ctx_kv, "sp", [code for code in sp_bits[::-1] if code not in raw_codes]
    )

    def attend(lat, lat_kinds, ctx, prev, is_last):
        shape = (tokens, cols)
        one = jax.ShapeDtypeStruct(shape, BF16)
        three = (jax.ShapeDtypeStruct(shape, F32),) * 3
        operands = [queries, *lat, *ctx] + ([tables] if lat else []) + list(prev)
        return call(
            functools.partial(
                attend_body, heads, lat_kinds, len(ctx), bool(prev), is_last
            ),
            out_shape=one if is_last else three,
            in_specs=vmem(len(operands)),
            out_specs=vmem(1)[0] if is_last else tuple(vmem(3)),
            compiler_params=params(24),
            cost_estimate=pl.CostEstimate(
                flops=1 << 37, bytes_accessed=1 << 20, transcendentals=0
            ),
        )(*operands)

    state = attend([kv], (OWN,), ctx_pieces[:1], (), False)
    attended = attend([near_kv, other_kv], (NEAR, OTHER), ctx_pieces[1:], state, True)

    att_blocks = gather_tp(attended, tp_bits)
    near = [n for n, (code, _) in enumerate(att_blocks) if code < 2]
    far = [n for n in range(len(att_blocks)) if n not in near]
    tile = min(512, width)
    att_spec = pl.BlockSpec((tokens, cols), lambda n: (0, 0))
    weight_spec = pl.BlockSpec((cols, tile), lambda n: (0, n))
    wide_spec = pl.BlockSpec((tokens, tile), lambda n: (0, n))
    kept = [n for n, (code, _) in enumerate(ow_blocks) if code in (0, 1) + tuple(code for code in tp_bits if code > 1)]
    stashed = call(
        stash_body,
        out_shape=tuple(jax.ShapeDtypeStruct((cols, width), BF16) for _ in kept),
        in_specs=raw(len(kept)),
        out_specs=tuple(vmem(len(kept))),
        scratch_shapes=[pltpu.SemaphoreType.DMA((len(kept),))],
        compiler_params=params(8),
    )(*[in_hbm(ow_blocks[n][1]) for n in kept])
    for n, w in zip(kept, stashed):
        ow_blocks[n] = (ow_blocks[n][0], w)
    partial_sum = call(
        functools.partial(first_body, len(near)),
        grid=(width // tile,),
        out_shape=jax.ShapeDtypeStruct((tokens, width), F32),
        in_specs=[att_spec] * len(near) + [weight_spec] * len(near),
        out_specs=wide_spec,
        compiler_params=params(24),
    )(*[att_blocks[n][1] for n in near], *[ow_blocks[n][1] for n in near])
    return call(
        functools.partial(output_body, len(far)),
        grid=(width // tile,),
        out_shape=jax.ShapeDtypeStruct((tokens, width), BF16),
        in_specs=[wide_spec, pl.BlockSpec((1, tile), lambda n: (0, n)), wide_spec]
        + [att_spec] * len(far)
        + [weight_spec] * len(far),
        out_specs=wide_spec,
        compiler_params=params(24),
    )(
        latent,
        gate,
        partial_sum,
        *[att_blocks[n][1] for n in far],
        *[ow_blocks[n][1] for n in far],
    )


RAW_CODES = (1,)


def solution(mesh):
    in_specs = (
        P("sp", None),
        P("sp", None),
        P("sp"),
        P("sp"),
        P("sp", "tp"),
        P("sp", "tp"),
        P("sp", "tp"),
        P(),
        P(None, "tp"),
        P(None, "tp"),
        P(None, "tp"),
        P(),
        P(),
        P("tp", None, None),
        P("tp", None),
    )
    out_specs = P("sp", None)
    return jax.shard_map(
        per_device, mesh=mesh, in_specs=in_specs, out_specs=out_specs, check_vma=False
    )
```

```python
import functools

import jax
import jax.numpy as jnp
from jax import lax
from jax.experimental import pallas as pl
from jax.experimental.pallas import tpu as pltpu
from jax.sharding import PartitionSpec as P


HEAD_DIM = 64
GRID_W = 64
WIN_ROWS = 8
WIN_COLS = 16
LANES = 128
EPS = 1e-06
MASKED = -1e30

F32 = jnp.float32
BF16 = jnp.bfloat16


def vmem(count):
    return [pl.BlockSpec(memory_space=pltpu.VMEM) for _ in range(count)]


def params(mib):
    return pltpu.CompilerParams(vmem_limit_bytes=mib << 20)


def swap(x, axis, code):
    return lax.ppermute(x, axis, [(i, i ^ code) for i in range(lax.axis_size(axis))])


def call(*args, **kwargs):
    def run(*operands):
        return pl.pallas_call(*args, **kwargs)(*operands)

    return run


def in_hbm(x):
    return pltpu.with_memory_space_constraint(x, pltpu.HBM)


def raw(count):
    return [pl.BlockSpec(memory_space=pltpu.HBM) for _ in range(count)]


def bits_of(axis):
    count = lax.axis_size(axis)
    return [1 << b for b in range(count.bit_length() - 1)]


def bt_dot(a, b):
    return lax.dot_general(a, b, (((1,), (1,)), ((), ())), preferred_element_type=F32)


def partials_body(
    cond_ref, ctx_cond_ref, shift_ref, scale_ref, gate_ref, ctx_ref, lat_ref,
    out_ref, ctx_half_ref, lat_half_ref, rows_ref, *scratch
):
    weights, sems = scratch[:3], scratch[3]
    half = ctx_half_ref.shape[1]
    at = pl.multiple_of(lax.rem(lax.axis_index("tp"), 2) * half, half)
    copies = [
        pltpu.make_async_copy(src, dst, sems.at[n])
        for n, (src, dst) in enumerate(
            (
                (cond_ref, rows_ref.at[0:1]),
                (ctx_cond_ref, rows_ref.at[1:2]),
                (shift_ref, weights[0]),
                (scale_ref, weights[1]),
                (gate_ref, weights[2]),
                (ctx_ref.at[:, pl.ds(at, half)], ctx_half_ref),
                (lat_ref.at[:, pl.ds(at, half)], lat_half_ref),
            )
        )
    ]
    for copy in copies:
        copy.start()
    copies[0].wait()
    copies[1].wait()
    rows = rows_ref[...]
    act = (rows / (1.0 + jnp.exp(-rows))).astype(BF16)
    for n in range(3):
        copies[2 + n].wait()
        out_ref[2 * n : 2 * n + 2, :] = jnp.dot(
            act, weights[n][...], preferred_element_type=F32
        )
    out_ref[6:8, :] = jnp.zeros((2, out_ref.shape[1]), F32)
    copies[5].wait()
    copies[6].wait()


def table_body(bias_ref, out_ref):
    heads, pairs = out_ref.shape[:2]
    q = lax.broadcasted_iota(jnp.int32, (GRID_W, 2 * GRID_W), 0)
    lane = lax.broadcasted_iota(jnp.int32, (GRID_W, 2 * GRID_W), 1)
    k = lane & (GRID_W - 1)
    start = jnp.clip(q - WIN_COLS // 2, 0, GRID_W - WIN_COLS)
    is_open = (k >= start) & (k < start + WIN_COLS)
    low = lane < GRID_W
    width = 2 * GRID_W
    for h in range(heads):
        rolled = []
        for a in range(pairs + 1):
            row = jnp.broadcast_to(bias_ref[h, a : a + 1, :], (GRID_W, width))
            rolled.append(row)
        for a in range(pairs):
            first = pltpu.roll(rolled[a], (1 - WIN_COLS) % width, 1, stride=1, stride_axis=0)
            second = pltpu.roll(
                rolled[a + 1], (1 - WIN_COLS + GRID_W) % width, 1, stride=1, stride_axis=0
            )
            out_ref[h, a] = jnp.where(is_open, jnp.where(low, first, second), MASKED)


def head_norm(x, gain_row):
    cols = x.shape[1]
    r = lax.broadcasted_iota(jnp.int32, (cols, cols), 0) // HEAD_DIM
    c = lax.broadcasted_iota(jnp.int32, (cols, cols), 1) // HEAD_DIM
    same = jnp.where(r == c, 1.0 / HEAD_DIM, 0.0).astype(BF16)
    head_gain = jnp.concatenate([gain_row[...]] * (cols // HEAD_DIM), axis=1)
    square = x * x
    high = square.astype(BF16)
    rest = (square - high.astype(F32)).astype(BF16)
    mean = jnp.dot(high, same, preferred_element_type=F32) + jnp.dot(
        rest, same, preferred_element_type=F32
    )
    return x * lax.rsqrt(mean + EPS) * head_gain


def modulated(values, vec_ref, gain_ref, row):
    mult = gain_ref[...] * (1.0 + vec_ref[2 + row : 3 + row, :])
    shift = vec_ref[row : row + 1, :]
    mean = jnp.mean(values * values, axis=-1, keepdims=True)
    return (values * lax.rsqrt(mean + EPS) * mult + shift).astype(BF16)


def join_halves(mine_ref, passed_ref, out_ref):
    half = mine_ref.shape[1]
    core = lax.rem(lax.axis_index("tp"), 2)
    out_ref[:, pl.ds(pl.multiple_of(core * half, half), half)] = mine_ref[...]
    out_ref[:, pl.ds(pl.multiple_of((1 - core) * half, half), half)] = passed_ref[...]


def row_steps(count):
    step = 32 if count % 32 == 0 else count
    return [slice(at, at + step) for at in range(0, count, step)]


def project_body(codes, lat_ref, ctx_ref, mine_ref, passed_ref, part_ref, beside_ref, *refs):
    gain_ref, kg_ref, wk, wv = refs[:4]
    kv_ref, ckv_ref, lat_hid_ref, vec_ref = refs[4:8]
    hid_ref, ctx_two_ref = refs[8:]
    width = part_ref.shape[1]
    me = lax.axis_index("tp")
    for n, code in enumerate(codes):
        for ref, flip in ((part_ref, 0), (beside_ref, 1)):
            at = pl.multiple_of((me ^ code ^ flip) * width, width)
            vec_ref[:, pl.ds(at, width)] = ref[8 * n : 8 * n + 8, :]
    join_halves(mine_ref, passed_ref, ctx_two_ref)
    lat_count = lat_ref.shape[0]
    ctx_count = ctx_ref.shape[0]
    for here in row_steps(lat_count):
        hid_ref[here, :] = modulated(lat_ref[here, :].astype(F32), vec_ref, gain_ref, 0)
    if ctx_count % 32:
        both = jnp.concatenate(
            [ctx_ref[...].astype(F32), ctx_two_ref[...].astype(F32)], axis=0
        )
        hid_ref[lat_count:, :] = modulated(both, vec_ref, gain_ref, 1)
    else:
        for n, ref in enumerate((ctx_ref, ctx_two_ref)):
            base = lat_count + n * ctx_count
            for here in row_steps(ctx_count):
                hid_ref[base + here.start : base + here.stop, :] = modulated(
                    ref[here, :].astype(F32), vec_ref, gain_ref, 1
                )
    cols = wk.shape[1]
    hidden = hid_ref[...]
    keys = head_norm(jnp.dot(hidden, wk[...], preferred_element_type=F32), kg_ref).astype(BF16)
    kv_ref[:, :cols] = keys[:lat_count]
    ckv_ref[:, :cols] = keys[lat_count:]
    values = jnp.dot(hidden, wv[...], preferred_element_type=F32).astype(BF16)
    kv_ref[:, cols:] = values[:lat_count]
    ckv_ref[:, cols:] = values[lat_count:]
    lat_hid_ref[...] = hidden[:lat_count]


def near_body(mine_ref, passed_ref, vec_ref, gain_ref, kg_ref, wk, wv, kv_ref, lat_ref, hid_ref):
    join_halves(mine_ref, passed_ref, lat_ref)
    for here in row_steps(lat_ref.shape[0]):
        hid_ref[here, :] = modulated(lat_ref[here, :].astype(F32), vec_ref, gain_ref, 0)
    cols = wk.shape[1]
    hidden = hid_ref[...]
    kv_ref[:, :cols] = head_norm(
        jnp.dot(hidden, wk[...], preferred_element_type=F32), kg_ref
    ).astype(BF16)
    kv_ref[:, cols:] = jnp.dot(hidden, wv[...], preferred_element_type=F32).astype(BF16)


def query_body(hid_ref, wq_ref, qg_ref, q_ref):
    queries = head_norm(
        jnp.dot(hid_ref[...], wq_ref[...], preferred_element_type=F32), qg_ref
    ).astype(BF16)
    q_ref[...] = (queries.astype(F32) * HEAD_DIM ** (-0.5)).astype(BF16)


OWN, NEAR, OTHER = range(3)


def attend_body(heads, lat_kinds, n_ctx, has_prev, is_last, q_ref, *refs):
    n_lat = len(lat_kinds)
    lat_refs, refs = refs[:n_lat], refs[n_lat:]
    ctx_refs, refs = refs[:n_ctx], refs[n_ctx:]
    if n_lat:
        table_ref, refs = refs[0], refs[1:]
    if has_prev:
        prev, refs = refs[:3], refs[3:]
    tokens, cols = q_ref.shape
    rows = tokens // GRID_W
    halo = WIN_ROWS // 2
    lane_head = lax.broadcasted_iota(jnp.int32, (1, cols), 1) // HEAD_DIM
    lane_row = lax.broadcasted_iota(jnp.int32, (1, 2 * GRID_W), 1) // GRID_W
    q_all = q_ref[...]
    parts = list(lat_refs) + list(ctx_refs)
    keys = [p[:, :cols] for p in parts]
    values = [p[:, cols:] for p in parts]
    sp_index = lax.axis_index("sp")
    first_row = sp_index * rows
    total_rows = rows * lax.axis_size("sp")
    starts = [
        jnp.clip(first_row + i - halo, 0, total_rows - WIN_ROWS) - first_row + halo
        for i in range(rows)
    ]
    is_odd = lax.rem(sp_index, 2)
    base_of = {
        OWN: halo,
        NEAR: (1 - is_odd) * (halo + rows),
        OTHER: is_odd * (halo + rows),
    }
    bases = [base_of[kind] for kind in lat_kinds]
    opens = {}
    for n in range(n_lat):
        for i in range(rows):
            for p in range(lat_refs[n].shape[0] // (2 * GRID_W)):
                row = lane_row + (bases[n] + 2 * p)
                start = starts[i]
                opens[n, i, p] = jnp.where(
                    (row >= start) & (row < start + WIN_ROWS), 0.0, MASKED
                )
    tops = jnp.zeros((tokens, cols), F32)
    sums = jnp.zeros((tokens, cols), F32)
    total = jnp.zeros((tokens, cols), F32)
    for h in range(heads):
        mine = lane_head == h
        q_h = jnp.where(mine, q_all, jnp.zeros_like(q_all))
        scores = [bt_dot(q_h, k) for k in keys]
        for n in range(n_lat):
            lines = []
            for i in range(rows):
                line = []
                for p in range(lat_refs[n].shape[0] // (2 * GRID_W)):
                    at = bases[n] + 2 * p - i + WIN_ROWS - 1 - halo
                    piece = scores[n][
                        i * GRID_W : (i + 1) * GRID_W, 2 * p * GRID_W : (2 * p + 2) * GRID_W
                    ]
                    line.append(piece + (table_ref[h, at] + opens[n, i, p]))
                lines.append(jnp.concatenate(line, axis=1))
            scores[n] = jnp.concatenate(lines, axis=0)
        top = functools.reduce(jnp.maximum, [jnp.max(s, axis=1, keepdims=True) for s in scores])
        powers = [jnp.exp(s - top) for s in scores]
        denom = functools.reduce(jnp.add, [jnp.sum(e, axis=1, keepdims=True) for e in powers])
        acc = functools.reduce(
            jnp.add,
            [
                jnp.dot(e.astype(BF16), v, preferred_element_type=F32)
                for e, v in zip(powers, values)
            ],
        )
        tops = jnp.where(mine, top, tops)
        sums = jnp.where(mine, denom, sums)
        total = jnp.where(mine, acc, total)
    if has_prev:
        before = prev[0][...]
        both = jnp.maximum(before, tops)
        old = jnp.exp(before - both)
        new = jnp.exp(tops - both)
        tops = both
        sums = prev[1][...] * old + sums * new
        total = prev[2][...] * old + total * new
    if is_last:
        refs[0][...] = (total / sums).astype(BF16)
    else:
        for ref, value in zip(refs, (tops, sums, total)):
            ref[...] = value


def stash_body(*refs):
    count = len(refs) // 2
    sems = refs[-1]
    copies = [
        pltpu.make_async_copy(src, dst, sems.at[n])
        for n, (src, dst) in enumerate(zip(refs[:count], refs[count : 2 * count]))
    ]
    for copy in copies:
        copy.start()
    for copy in copies:
        copy.wait()


def first_body(count, has_prev, *refs):
    branch = None
    if has_prev:
        branch, refs = refs[0][...], refs[1:]
    att, weights, sum_ref = refs[:count], refs[count : 2 * count], refs[2 * count]
    for a, w in zip(att, weights):
        part = jnp.dot(a[...], w[...], preferred_element_type=F32).astype(BF16).astype(F32)
        branch = part if branch is None else branch + part
    sum_ref[...] = branch


def output_body(count, lat_ref, gate_ref, sum_ref, *refs):
    att = refs[:count]
    weights = refs[count : 2 * count]
    out_ref = refs[2 * count]
    branch = sum_ref[...]
    for a, w in zip(att, weights):
        branch = branch + jnp.dot(a[...], w[...], preferred_element_type=F32).astype(
            BF16
        ).astype(F32)
    out_ref[...] = (lat_ref[...].astype(F32) + gate_ref[4:5, :] * branch).astype(BF16)


def gather_pieces(x, axis, codes):
    pieces = [x]
    for code in codes:
        if len(pieces) > 2:
            pieces = [jnp.concatenate(pieces, axis=0)]
        pieces = pieces + [swap(p, axis, code) for p in pieces]
    return pieces


def gather_tp(x, codes):
    held = [(0, x)]
    for code in codes:
        held = held + [(had ^ code, swap(p, "tp", code)) for had, p in held]
    return held


def per_device(
    latent,
    context,
    condition,
    ctx_condition,
    shift_weight,
    scale_weight,
    gate_weight,
    norm_gain,
    query_weight,
    key_weight,
    value_weight,
    query_gain,
    key_gain,
    offset_bias,
    out_weight,
):
    sp_bits = bits_of("sp")
    tp_bits = bits_of("tp")[::-1]
    tokens, width = latent.shape
    cols = query_weight.shape[1]
    heads = cols // HEAD_DIM
    block_cols = shift_weight.shape[1]

    half = width // 2
    part, ctx_half, lat_half = call(
        partials_body,
        out_shape=(
            jax.ShapeDtypeStruct((8, block_cols), F32),
            jax.ShapeDtypeStruct((context.shape[0], half), BF16),
            jax.ShapeDtypeStruct((tokens, half), BF16),
        ),
        in_specs=raw(7),
        out_specs=tuple(vmem(3)),
        scratch_shapes=[pltpu.VMEM((2, condition.shape[0]), F32)]
        + [pltpu.VMEM(shift_weight.shape, BF16)] * 3
        + [pltpu.SemaphoreType.DMA((7,))],
        compiler_params=params(16),
        cost_estimate=pl.CostEstimate(flops=1 << 37, bytes_accessed=1 << 20, transcendentals=0),
    )(
        *[
            in_hbm(x)
            for x in (
                condition[None],
                ctx_condition[None],
                shift_weight,
                scale_weight,
                gate_weight,
                context,
                latent,
            )
        ]
    )
    raw_code = sp_bits[min(2, len(sp_bits) - 1)]
    ctx_mine = swap(ctx_half, "sp", raw_code)
    ctx_passed = swap(ctx_mine, "tp", 1)
    near_mine = swap(lat_half, "sp", 1)
    near_passed = swap(near_mine, "tp", 1)
    codes = [0]
    for code in tp_bits:
        if code > 1:
            part = jnp.concatenate([part, swap(part, "tp", code)], axis=0)
            codes = codes + [had ^ code for had in codes]
    for code in sp_bits:
        part = part + swap(part, "sp", code)
    beside = swap(part, "tp", 1)
    ow_blocks = gather_tp(out_weight, tp_bits)

    padded_bias = jnp.pad(offset_bias, ((0, 0), (0, 0), (0, LANES - offset_bias.shape[2])))
    tables = call(
        table_body,
        out_shape=jax.ShapeDtypeStruct((heads, 2 * WIN_ROWS - 2, GRID_W, 2 * GRID_W), F32),
        in_specs=vmem(1),
        out_specs=vmem(1)[0],
        compiler_params=params(16),
    )(padded_bias)

    ctx_count = 2 * context.shape[0]
    gain = norm_gain[None]
    kv, ctx_kv, hidden, vec = call(
        functools.partial(project_body, tuple(codes)),
        out_shape=(
            jax.ShapeDtypeStruct((tokens, 2 * cols), BF16),
            jax.ShapeDtypeStruct((ctx_count, 2 * cols), BF16),
            jax.ShapeDtypeStruct((tokens, width), BF16),
            jax.ShapeDtypeStruct((8, width), F32),
        ),
        in_specs=vmem(10),
        out_specs=vmem(4),
        scratch_shapes=[
            pltpu.VMEM((tokens + ctx_count, width), BF16),
            pltpu.VMEM(context.shape, BF16),
        ],
        compiler_params=params(20),
        cost_estimate=pl.CostEstimate(flops=1 << 37, bytes_accessed=1 << 20, transcendentals=0),
    )(
        latent,
        context,
        ctx_mine,
        ctx_passed,
        part,
        beside,
        gain,
        key_gain[None],
        key_weight,
        value_weight,
    )
    near_kv = call(
        near_body,
        out_shape=jax.ShapeDtypeStruct((tokens, 2 * cols), BF16),
        in_specs=vmem(7),
        out_specs=vmem(1)[0],
        scratch_shapes=[pltpu.VMEM((tokens, width), BF16)] * 2,
        compiler_params=params(20),
    )(near_mine, near_passed, vec, gain, key_gain[None], key_weight, value_weight)
    queries = call(
        query_body,
        out_shape=jax.ShapeDtypeStruct((tokens, cols), BF16),
        in_specs=vmem(3),
        out_specs=vmem(1)[0],
        compiler_params=params(8),
    )(hidden, query_weight, query_gain[None])

    sp_count = lax.axis_size("sp")
    other_pairs = [(i, i + 1) for i in range(1, sp_count - 1, 2)]
    other_pairs += [(j, i) for i, j in other_pairs]
    other_kv = lax.ppermute(kv, "sp", other_pairs)
    ctx_pieces = gather_pieces(ctx_kv, "sp", [code for code in sp_bits if code != raw_code])

    def attend(lat, lat_kinds, ctx, prev, is_last):
        shape = (tokens, cols)
        one = jax.ShapeDtypeStruct(shape, BF16)
        three = (jax.ShapeDtypeStruct(shape, F32),) * 3
        operands = [queries, *lat, *ctx] + ([tables] if lat else []) + list(prev)
        return call(
            functools.partial(
                attend_body, heads, lat_kinds, len(ctx), bool(prev), is_last
            ),
            out_shape=one if is_last else three,
            in_specs=vmem(len(operands)),
            out_specs=vmem(1)[0] if is_last else tuple(vmem(3)),
            compiler_params=params(24),
            cost_estimate=pl.CostEstimate(
                flops=1 << 37, bytes_accessed=1 << 20, transcendentals=0
            ),
        )(*operands)

    state = attend([kv, near_kv], (OWN, NEAR), ctx_pieces[:1], (), False)
    attended = attend([other_kv], (OTHER,), ctx_pieces[1:], state, True)

    att_blocks = gather_tp(attended, tp_bits)

    def stash(index):
        code, w = ow_blocks[index]
        (held,) = call(
            stash_body,
            out_shape=(jax.ShapeDtypeStruct((cols, width), BF16),),
            in_specs=raw(1),
            out_specs=tuple(vmem(1)),
            scratch_shapes=[pltpu.SemaphoreType.DMA((1,))],
            compiler_params=params(8),
        )(in_hbm(w))
        ow_blocks[index] = (code, held)

    for n in range(len(ow_blocks) // 2):
        stash(n)

    near = [n for n, (code, _) in enumerate(att_blocks) if code < 2]
    cross = [n for n, (code, _) in enumerate(att_blocks) if code > 1 and n < len(att_blocks) // 2]
    far = [n for n in range(len(att_blocks)) if n not in near + cross]
    tile = min(512, width)
    att_spec = pl.BlockSpec((tokens, cols), lambda n: (0, 0))
    weight_spec = pl.BlockSpec((cols, tile), lambda n: (0, n))
    wide_spec = pl.BlockSpec((tokens, tile), lambda n: (0, n))

    def operands(which):
        return [att_blocks[n][1] for n in which] + [ow_blocks[n][1] for n in which]

    def specs(which):
        return [att_spec] * len(which) + [weight_spec] * len(which)

    partial_sum = call(
        functools.partial(first_body, len(near), False),
        grid=(width // tile,),
        out_shape=jax.ShapeDtypeStruct((tokens, width), F32),
        in_specs=specs(near),
        out_specs=wide_spec,
        compiler_params=params(24),
    )(*operands(near))
    partial_sum = call(
        functools.partial(first_body, len(cross), True),
        grid=(width // tile,),
        out_shape=jax.ShapeDtypeStruct((tokens, width), F32),
        in_specs=[wide_spec] + specs(cross),
        out_specs=wide_spec,
        compiler_params=params(24),
    )(partial_sum, *operands(cross))
    return call(
        functools.partial(output_body, len(far)),
        grid=(width // tile,),
        out_shape=jax.ShapeDtypeStruct((tokens, width), BF16),
        in_specs=[wide_spec, pl.BlockSpec((8, tile), lambda n: (0, n)), wide_spec]
        + specs(far),
        out_specs=wide_spec,
        compiler_params=params(24),
    )(latent, vec, partial_sum, *operands(far))


def solution(mesh):
    in_specs = (
        P("sp", None),
        P("sp", None),
        P("sp"),
        P("sp"),
        P("sp", "tp"),
        P("sp", "tp"),
        P("sp", "tp"),
        P(),
        P(None, "tp"),
        P(None, "tp"),
        P(None, "tp"),
        P(),
        P(),
        P("tp", None, None),
        P("tp", None),
    )
    out_specs = P("sp", None)
    return jax.shard_map(
        per_device, mesh=mesh, in_specs=in_specs, out_specs=out_specs, check_vma=False
    )
```

```python
import functools

import jax
import jax.numpy as jnp
from jax import lax
from jax.experimental import pallas as pl
from jax.experimental.pallas import tpu as pltpu
from jax.sharding import PartitionSpec as P


HEAD_DIM = 64
GRID_W = 64
WIN_ROWS = 8
WIN_COLS = 16
LANES = 128
EPS = 1e-06
MASKED = -1e30

F32 = jnp.float32
BF16 = jnp.bfloat16


def vmem(count):
    return [pl.BlockSpec(memory_space=pltpu.VMEM) for _ in range(count)]


def params(mib):
    return pltpu.CompilerParams(vmem_limit_bytes=mib << 20)


def swap(x, axis, code):
    return lax.ppermute(x, axis, [(i, i ^ code) for i in range(lax.axis_size(axis))])


def call(*args, **kwargs):
    def run(*operands):
        return pl.pallas_call(*args, **kwargs)(*operands)

    return run


def in_hbm(x):
    return pltpu.with_memory_space_constraint(x, pltpu.HBM)


def raw(count):
    return [pl.BlockSpec(memory_space=pltpu.HBM) for _ in range(count)]


def bits_of(axis):
    count = lax.axis_size(axis)
    return [1 << b for b in range(count.bit_length() - 1)]


def bt_dot(a, b):
    return lax.dot_general(a, b, (((1,), (1,)), ((), ())), preferred_element_type=F32)


def partials_body(
    cond_ref, ctx_cond_ref, shift_ref, scale_ref, gate_ref, ctx_ref, lat_ref,
    out_ref, ctx_half_ref, lat_half_ref, rows_ref, *scratch
):
    weights, sems = scratch[:3], scratch[3]
    half = ctx_half_ref.shape[1]
    at = pl.multiple_of(lax.rem(lax.axis_index("tp"), 2) * half, half)
    copies = [
        pltpu.make_async_copy(src, dst, sems.at[n])
        for n, (src, dst) in enumerate(
            (
                (cond_ref, rows_ref.at[0:1]),
                (ctx_cond_ref, rows_ref.at[1:2]),
                (shift_ref, weights[0]),
                (scale_ref, weights[1]),
                (gate_ref, weights[2]),
                (ctx_ref.at[:, pl.ds(at, half)], ctx_half_ref),
                (lat_ref.at[:, pl.ds(at, half)], lat_half_ref),
            )
        )
    ]
    for copy in copies:
        copy.start()
    copies[0].wait()
    copies[1].wait()
    rows = rows_ref[...]
    act = (rows / (1.0 + jnp.exp(-rows))).astype(BF16)
    for n in range(3):
        copies[2 + n].wait()
        out_ref[2 * n : 2 * n + 2, :] = jnp.dot(
            act, weights[n][...], preferred_element_type=F32
        )
    out_ref[6:8, :] = jnp.zeros((2, out_ref.shape[1]), F32)
    copies[5].wait()
    copies[6].wait()


def table_body(bias_ref, out_ref):
    heads, pairs = out_ref.shape[:2]
    q = lax.broadcasted_iota(jnp.int32, (GRID_W, 2 * GRID_W), 0)
    lane = lax.broadcasted_iota(jnp.int32, (GRID_W, 2 * GRID_W), 1)
    k = lane & (GRID_W - 1)
    start = jnp.clip(q - WIN_COLS // 2, 0, GRID_W - WIN_COLS)
    is_open = (k >= start) & (k < start + WIN_COLS)
    low = lane < GRID_W
    width = 2 * GRID_W
    for h in range(heads):
        rolled = []
        for a in range(pairs + 1):
            row = jnp.broadcast_to(bias_ref[h, a : a + 1, :], (GRID_W, width))
            rolled.append(row)
        for a in range(pairs):
            first = pltpu.roll(rolled[a], (1 - WIN_COLS) % width, 1, stride=1, stride_axis=0)
            second = pltpu.roll(
                rolled[a + 1], (1 - WIN_COLS + GRID_W) % width, 1, stride=1, stride_axis=0
            )
            out_ref[h, a] = jnp.where(is_open, jnp.where(low, first, second), MASKED)


def head_norm(x, gain_row):
    cols = x.shape[1]
    r = lax.broadcasted_iota(jnp.int32, (cols, cols), 0) // HEAD_DIM
    c = lax.broadcasted_iota(jnp.int32, (cols, cols), 1) // HEAD_DIM
    same = jnp.where(r == c, 1.0 / HEAD_DIM, 0.0).astype(BF16)
    head_gain = jnp.concatenate([gain_row[...]] * (cols // HEAD_DIM), axis=1)
    square = x * x
    high = square.astype(BF16)
    rest = (square - high.astype(F32)).astype(BF16)
    mean = jnp.dot(high, same, preferred_element_type=F32) + jnp.dot(
        rest, same, preferred_element_type=F32
    )
    return x * lax.rsqrt(mean + EPS) * head_gain


def modulated(values, vec_ref, gain_ref, row):
    mult = gain_ref[...] * (1.0 + vec_ref[2 + row : 3 + row, :])
    shift = vec_ref[row : row + 1, :]
    mean = jnp.mean(values * values, axis=-1, keepdims=True)
    return (values * lax.rsqrt(mean + EPS) * mult + shift).astype(BF16)


def join_halves(mine_ref, passed_ref, out_ref):
    half = mine_ref.shape[1]
    core = lax.rem(lax.axis_index("tp"), 2)
    out_ref[:, pl.ds(pl.multiple_of(core * half, half), half)] = mine_ref[...]
    out_ref[:, pl.ds(pl.multiple_of((1 - core) * half, half), half)] = passed_ref[...]


def row_steps(count):
    step = 32 if count % 32 == 0 else count
    return [slice(at, at + step) for at in range(0, count, step)]


def project_body(codes, lat_ref, ctx_ref, mine_ref, passed_ref, part_ref, beside_ref, *refs):
    gain_ref, kg_ref, wk, wv = refs[:4]
    kv_ref, ckv_ref, lat_hid_ref, vec_ref = refs[4:8]
    hid_ref, ctx_two_ref = refs[8:]
    width = part_ref.shape[1]
    me = lax.axis_index("tp")
    for n, code in enumerate(codes):
        for ref, flip in ((part_ref, 0), (beside_ref, 1)):
            at = pl.multiple_of((me ^ code ^ flip) * width, width)
            vec_ref[:, pl.ds(at, width)] = ref[8 * n : 8 * n + 8, :]
    join_halves(mine_ref, passed_ref, ctx_two_ref)
    lat_count = lat_ref.shape[0]
    ctx_count = ctx_ref.shape[0]
    for here in row_steps(lat_count):
        lat_hid_ref[here, :] = modulated(lat_ref[here, :].astype(F32), vec_ref, gain_ref, 0)
    if ctx_count % 32:
        both = jnp.concatenate(
            [ctx_ref[...].astype(F32), ctx_two_ref[...].astype(F32)], axis=0
        )
        hid_ref[...] = modulated(both, vec_ref, gain_ref, 1)
    else:
        for n, ref in enumerate((ctx_ref, ctx_two_ref)):
            base = n * ctx_count
            for here in row_steps(ctx_count):
                hid_ref[base + here.start : base + here.stop, :] = modulated(
                    ref[here, :].astype(F32), vec_ref, gain_ref, 1
                )
    cols = wk.shape[1]
    for out, src in ((kv_ref, lat_hid_ref[...]), (ckv_ref, hid_ref[...])):
        out[:, :cols] = head_norm(
            jnp.dot(src, wk[...], preferred_element_type=F32), kg_ref
        ).astype(BF16)
        out[:, cols:] = jnp.dot(src, wv[...], preferred_element_type=F32).astype(BF16)


def near_body(mine_ref, passed_ref, vec_ref, gain_ref, kg_ref, wk, wv, kv_ref, lat_ref, hid_ref):
    join_halves(mine_ref, passed_ref, lat_ref)
    for here in row_steps(lat_ref.shape[0]):
        hid_ref[here, :] = modulated(lat_ref[here, :].astype(F32), vec_ref, gain_ref, 0)
    cols = wk.shape[1]
    step = lat_ref.shape[0] // 2
    for at in range(0, lat_ref.shape[0], step):
        hidden = hid_ref[at : at + step, :]
        kv_ref[at : at + step, :cols] = head_norm(
            jnp.dot(hidden, wk[...], preferred_element_type=F32), kg_ref
        ).astype(BF16)
        kv_ref[at : at + step, cols:] = jnp.dot(
            hidden, wv[...], preferred_element_type=F32
        ).astype(BF16)


def query_body(hid_ref, wq_ref, qg_ref, q_ref):
    queries = head_norm(
        jnp.dot(hid_ref[...], wq_ref[...], preferred_element_type=F32), qg_ref
    ).astype(BF16)
    q_ref[...] = (queries.astype(F32) * HEAD_DIM ** (-0.5)).astype(BF16)


OWN, NEAR, OTHER = range(3)


def attend_body(heads, lat_kinds, n_ctx, has_prev, is_last, q_ref, *refs):
    n_lat = len(lat_kinds)
    lat_refs, refs = refs[:n_lat], refs[n_lat:]
    ctx_refs, refs = refs[:n_ctx], refs[n_ctx:]
    if n_lat:
        table_ref, refs = refs[0], refs[1:]
    if has_prev:
        prev, refs = refs[:3], refs[3:]
    tokens, cols = q_ref.shape
    rows = tokens // GRID_W
    halo = WIN_ROWS // 2
    lane_head = lax.broadcasted_iota(jnp.int32, (1, cols), 1) // HEAD_DIM
    lane_row = lax.broadcasted_iota(jnp.int32, (1, 2 * GRID_W), 1) // GRID_W
    q_all = q_ref[...]
    parts = list(lat_refs) + list(ctx_refs)
    keys = [p[:, :cols] for p in parts]
    values = [p[:, cols:] for p in parts]
    sp_index = lax.axis_index("sp")
    first_row = sp_index * rows
    total_rows = rows * lax.axis_size("sp")
    starts = [
        jnp.clip(first_row + i - halo, 0, total_rows - WIN_ROWS) - first_row + halo
        for i in range(rows)
    ]
    is_odd = lax.rem(sp_index, 2)
    base_of = {
        OWN: halo,
        NEAR: (1 - is_odd) * (halo + rows),
        OTHER: is_odd * (halo + rows),
    }
    bases = [base_of[kind] for kind in lat_kinds]
    opens = {}
    for n in range(n_lat):
        for i in range(rows):
            for p in range(lat_refs[n].shape[0] // (2 * GRID_W)):
                row = lane_row + (bases[n] + 2 * p)
                start = starts[i]
                opens[n, i, p] = jnp.where(
                    (row >= start) & (row < start + WIN_ROWS), 0.0, MASKED
                )
    masks = [lane_head == h for h in range(heads)]
    all_scores = []
    for mine in masks:
        q_h = jnp.where(mine, q_all, jnp.zeros_like(q_all))
        all_scores.append([bt_dot(q_h, k) for k in keys])
    all_powers, tops, sums = [], None, None
    for h, scores in enumerate(all_scores):
        for n in range(n_lat):
            lines = []
            for i in range(rows):
                line = []
                for p in range(lat_refs[n].shape[0] // (2 * GRID_W)):
                    at = bases[n] + 2 * p - i + WIN_ROWS - 1 - halo
                    piece = scores[n][
                        i * GRID_W : (i + 1) * GRID_W, 2 * p * GRID_W : (2 * p + 2) * GRID_W
                    ]
                    line.append(piece + (table_ref[h, at] + opens[n, i, p]))
                lines.append(jnp.concatenate(line, axis=1))
            scores[n] = jnp.concatenate(lines, axis=0)
        top = functools.reduce(jnp.maximum, [jnp.max(s, axis=1, keepdims=True) for s in scores])
        powers = [jnp.exp(s - top) for s in scores]
        denom = functools.reduce(jnp.add, [jnp.sum(e, axis=1, keepdims=True) for e in powers])
        all_powers.append([e.astype(BF16) for e in powers])
        tops = jnp.broadcast_to(top, (tokens, cols)) if h == 0 else jnp.where(masks[h], top, tops)
        sums = jnp.broadcast_to(denom, (tokens, cols)) if h == 0 else jnp.where(masks[h], denom, sums)
    total = None
    for h, powers in enumerate(all_powers):
        acc = functools.reduce(
            jnp.add,
            [jnp.dot(e, v, preferred_element_type=F32) for e, v in zip(powers, values)],
        )
        total = acc if h == 0 else jnp.where(masks[h], acc, total)
    if has_prev:
        before = prev[0][...]
        both = jnp.maximum(before, tops)
        old = jnp.exp(before - both)
        new = jnp.exp(tops - both)
        tops = both
        sums = prev[1][...] * old + sums * new
        total = prev[2][...] * old + total * new
    if is_last:
        refs[0][...] = (total / sums).astype(BF16)
    else:
        for ref, value in zip(refs, (tops, sums, total)):
            ref[...] = value


def stash_body(*refs):
    count = len(refs) // 2
    sems = refs[-1]
    copies = [
        pltpu.make_async_copy(src, dst, sems.at[n])
        for n, (src, dst) in enumerate(zip(refs[:count], refs[count : 2 * count]))
    ]
    for copy in copies:
        copy.start()
    for copy in copies:
        copy.wait()


def first_body(count, has_prev, *refs):
    branch = None
    if has_prev:
        branch, refs = refs[0][...], refs[1:]
    att, weights, sum_ref = refs[:count], refs[count : 2 * count], refs[2 * count]
    for a, w in zip(att, weights):
        part = jnp.dot(a[...], w[...], preferred_element_type=F32).astype(BF16).astype(F32)
        branch = part if branch is None else branch + part
    sum_ref[...] = branch


def output_body(count, lat_ref, gate_ref, sum_ref, *refs):
    att = refs[:count]
    weights = refs[count : 2 * count]
    out_ref = refs[2 * count]
    branch = sum_ref[...]
    for a, w in zip(att, weights):
        branch = branch + jnp.dot(a[...], w[...], preferred_element_type=F32).astype(
            BF16
        ).astype(F32)
    out_ref[...] = (lat_ref[...].astype(F32) + gate_ref[4:5, :] * branch).astype(BF16)


def gather_pieces(x, axis, codes):
    pieces = [x]
    for code in codes:
        if len(pieces) > 2:
            pieces = [jnp.concatenate(pieces, axis=0)]
        pieces = pieces + [swap(p, axis, code) for p in pieces]
    return pieces


def gather_tp(x, codes):
    held = [(0, x)]
    for code in codes:
        held = held + [(had ^ code, swap(p, "tp", code)) for had, p in held]
    return held


def per_device(
    latent,
    context,
    condition,
    ctx_condition,
    shift_weight,
    scale_weight,
    gate_weight,
    norm_gain,
    query_weight,
    key_weight,
    value_weight,
    query_gain,
    key_gain,
    offset_bias,
    out_weight,
):
    sp_bits = bits_of("sp")
    tp_bits = bits_of("tp")[::-1]
    tokens, width = latent.shape
    cols = query_weight.shape[1]
    heads = cols // HEAD_DIM
    block_cols = shift_weight.shape[1]

    half = width // 2
    part, ctx_half, lat_half = call(
        partials_body,
        out_shape=(
            jax.ShapeDtypeStruct((8, block_cols), F32),
            jax.ShapeDtypeStruct((context.shape[0], half), BF16),
            jax.ShapeDtypeStruct((tokens, half), BF16),
        ),
        in_specs=raw(7),
        out_specs=tuple(vmem(3)),
        scratch_shapes=[pltpu.VMEM((2, condition.shape[0]), F32)]
        + [pltpu.VMEM(shift_weight.shape, BF16)] * 3
        + [pltpu.SemaphoreType.DMA((7,))],
        compiler_params=params(16),
        cost_estimate=pl.CostEstimate(flops=1 << 37, bytes_accessed=1 << 20, transcendentals=0),
    )(
        *[
            in_hbm(x)
            for x in (
                condition[None],
                ctx_condition[None],
                shift_weight,
                scale_weight,
                gate_weight,
                context,
                latent,
            )
        ]
    )
    raw_code = sp_bits[min(2, len(sp_bits) - 1)]
    ctx_mine = swap(ctx_half, "sp", raw_code)
    ctx_passed = swap(ctx_mine, "tp", 1)
    near_mine = swap(lat_half, "sp", 1)
    near_passed = swap(near_mine, "tp", 1)
    codes = [0]
    for code in tp_bits:
        if code > 1:
            part = jnp.concatenate([part, swap(part, "tp", code)], axis=0)
            codes = codes + [had ^ code for had in codes]
    for code in sp_bits:
        part = part + swap(part, "sp", code)
    beside = swap(part, "tp", 1)
    ow_blocks = gather_tp(out_weight, tp_bits)

    padded_bias = jnp.pad(offset_bias, ((0, 0), (0, 0), (0, LANES - offset_bias.shape[2])))
    tables = call(
        table_body,
        out_shape=jax.ShapeDtypeStruct((heads, 2 * WIN_ROWS - 2, GRID_W, 2 * GRID_W), F32),
        in_specs=vmem(1),
        out_specs=vmem(1)[0],
        compiler_params=params(16),
    )(padded_bias)

    ctx_count = 2 * context.shape[0]
    gain = norm_gain[None]
    kv, ctx_kv, hidden, vec = call(
        functools.partial(project_body, tuple(codes)),
        out_shape=(
            jax.ShapeDtypeStruct((tokens, 2 * cols), BF16),
            jax.ShapeDtypeStruct((ctx_count, 2 * cols), BF16),
            jax.ShapeDtypeStruct((tokens, width), BF16),
            jax.ShapeDtypeStruct((8, width), F32),
        ),
        in_specs=vmem(10),
        out_specs=vmem(4),
        scratch_shapes=[
            pltpu.VMEM((ctx_count, width), BF16),
            pltpu.VMEM(context.shape, BF16),
        ],
        compiler_params=params(20),
        cost_estimate=pl.CostEstimate(flops=1 << 37, bytes_accessed=1 << 20, transcendentals=0),
    )(
        latent,
        context,
        ctx_mine,
        ctx_passed,
        part,
        beside,
        gain,
        key_gain[None],
        key_weight,
        value_weight,
    )
    near_kv = call(
        near_body,
        out_shape=jax.ShapeDtypeStruct((tokens, 2 * cols), BF16),
        in_specs=vmem(7),
        out_specs=vmem(1)[0],
        scratch_shapes=[pltpu.VMEM((tokens, width), BF16)] * 2,
        compiler_params=params(20),
    )(near_mine, near_passed, vec, gain, key_gain[None], key_weight, value_weight)
    queries = call(
        query_body,
        out_shape=jax.ShapeDtypeStruct((tokens, cols), BF16),
        in_specs=vmem(3),
        out_specs=vmem(1)[0],
        compiler_params=params(8),
    )(hidden, query_weight, query_gain[None])

    sp_count = lax.axis_size("sp")
    other_pairs = [(i, i + 1) for i in range(1, sp_count - 1, 2)]
    other_pairs += [(j, i) for i, j in other_pairs]
    other_kv = lax.ppermute(kv, "sp", other_pairs)
    ctx_pieces = gather_pieces(ctx_kv, "sp", [code for code in sp_bits if code != raw_code])

    def attend(lat, lat_kinds, ctx, prev, is_last):
        shape = (tokens, cols)
        one = jax.ShapeDtypeStruct(shape, BF16)
        three = (jax.ShapeDtypeStruct(shape, F32),) * 3
        operands = [queries, *lat, *ctx] + ([tables] if lat else []) + list(prev)
        return call(
            functools.partial(
                attend_body, heads, lat_kinds, len(ctx), bool(prev), is_last
            ),
            out_shape=one if is_last else three,
            in_specs=vmem(len(operands)),
            out_specs=vmem(1)[0] if is_last else tuple(vmem(3)),
            compiler_params=params(24),
            cost_estimate=pl.CostEstimate(
                flops=1 << 37, bytes_accessed=1 << 20, transcendentals=0
            ),
        )(*operands)

    state = attend([kv, near_kv], (OWN, NEAR), ctx_pieces[:1], (), False)
    attended = attend([other_kv], (OTHER,), ctx_pieces[1:], state, True)

    att_blocks = gather_tp(attended, tp_bits)

    def stash(index):
        code, w = ow_blocks[index]
        (held,) = call(
            stash_body,
            out_shape=(jax.ShapeDtypeStruct((cols, width), BF16),),
            in_specs=raw(1),
            out_specs=tuple(vmem(1)),
            scratch_shapes=[pltpu.SemaphoreType.DMA((1,))],
            compiler_params=params(8),
        )(in_hbm(w))
        ow_blocks[index] = (code, held)

    for n in range(len(ow_blocks) // 2):
        stash(n)

    near = [n for n, (code, _) in enumerate(att_blocks) if code < 2]
    cross = [n for n, (code, _) in enumerate(att_blocks) if code > 1 and n < len(att_blocks) // 2]
    far = [n for n in range(len(att_blocks)) if n not in near + cross]
    tile = min(1024, width)
    att_spec = pl.BlockSpec((tokens, cols), lambda n: (0, 0))
    weight_spec = pl.BlockSpec((cols, tile), lambda n: (0, n))
    wide_spec = pl.BlockSpec((tokens, tile), lambda n: (0, n))

    def operands(which):
        return [att_blocks[n][1] for n in which] + [ow_blocks[n][1] for n in which]

    def specs(which):
        return [att_spec] * len(which) + [weight_spec] * len(which)

    partial_sum = call(
        functools.partial(first_body, len(near), False),
        out_shape=jax.ShapeDtypeStruct((tokens, width), F32),
        in_specs=vmem(2 * len(near)),
        out_specs=vmem(1)[0],
        compiler_params=params(24),
    )(*operands(near))
    partial_sum = call(
        functools.partial(first_body, len(cross), True),
        out_shape=jax.ShapeDtypeStruct((tokens, width), F32),
        in_specs=vmem(1 + 2 * len(cross)),
        out_specs=vmem(1)[0],
        compiler_params=params(24),
    )(partial_sum, *operands(cross))
    return call(
        functools.partial(output_body, len(far)),
        grid=(width // tile,),
        out_shape=jax.ShapeDtypeStruct((tokens, width), BF16),
        in_specs=[wide_spec, pl.BlockSpec((8, tile), lambda n: (0, n)), wide_spec]
        + specs(far),
        out_specs=wide_spec,
        compiler_params=params(24),
    )(latent, vec, partial_sum, *operands(far))


def solution(mesh):
    in_specs = (
        P("sp", None),
        P("sp", None),
        P("sp"),
        P("sp"),
        P("sp", "tp"),
        P("sp", "tp"),
        P("sp", "tp"),
        P(),
        P(None, "tp"),
        P(None, "tp"),
        P(None, "tp"),
        P(),
        P(),
        P("tp", None, None),
        P("tp", None),
    )
    out_specs = P("sp", None)
    return jax.shard_map(
        per_device, mesh=mesh, in_specs=in_specs, out_specs=out_specs, check_vma=False
    )
```

```python
import functools

import jax
import jax.numpy as jnp
from jax import lax
from jax.experimental import pallas as pl
from jax.experimental.pallas import tpu as pltpu
from jax.sharding import PartitionSpec as P


HEAD_DIM = 64
GRID_W = 64
WIN_ROWS = 8
WIN_COLS = 16
LANES = 128
EPS = 1e-06
MASKED = -1e30

F32 = jnp.float32
BF16 = jnp.bfloat16


def vmem(count):
    return [pl.BlockSpec(memory_space=pltpu.VMEM) for _ in range(count)]


def params(mib):
    return pltpu.CompilerParams(vmem_limit_bytes=mib << 20)


def swap(x, axis, code):
    return lax.ppermute(x, axis, [(i, i ^ code) for i in range(lax.axis_size(axis))])


def call(*args, **kwargs):
    def run(*operands):
        return pl.pallas_call(*args, **kwargs)(*operands)

    return run


def in_hbm(x):
    return pltpu.with_memory_space_constraint(x, pltpu.HBM)


def raw(count):
    return [pl.BlockSpec(memory_space=pltpu.HBM) for _ in range(count)]


def bits_of(axis):
    count = lax.axis_size(axis)
    return [1 << b for b in range(count.bit_length() - 1)]


def bt_dot(a, b):
    return lax.dot_general(a, b, (((1,), (1,)), ((), ())), preferred_element_type=F32)


def partials_body(
    cond_ref, ctx_cond_ref, shift_ref, scale_ref, gate_ref, ctx_ref, lat_ref,
    out_ref, ctx_half_ref, lat_half_ref, rows_ref, *scratch
):
    weights, sems = scratch[:3], scratch[3]
    half = ctx_half_ref.shape[1]
    at = pl.multiple_of(lax.rem(lax.axis_index("tp"), 2) * half, half)
    copies = [
        pltpu.make_async_copy(src, dst, sems.at[n])
        for n, (src, dst) in enumerate(
            (
                (cond_ref, rows_ref.at[0:1]),
                (ctx_cond_ref, rows_ref.at[1:2]),
                (shift_ref, weights[0]),
                (scale_ref, weights[1]),
                (gate_ref, weights[2]),
                (ctx_ref.at[:, pl.ds(at, half)], ctx_half_ref),
                (lat_ref.at[:, pl.ds(at, half)], lat_half_ref),
            )
        )
    ]
    for copy in copies:
        copy.start()
    copies[0].wait()
    copies[1].wait()
    rows = rows_ref[...]
    act = (rows / (1.0 + jnp.exp(-rows))).astype(BF16)
    for n in range(3):
        copies[2 + n].wait()
        out_ref[2 * n : 2 * n + 2, :] = jnp.dot(
            act, weights[n][...], preferred_element_type=F32
        )
    out_ref[6:8, :] = jnp.zeros((2, out_ref.shape[1]), F32)
    copies[5].wait()
    copies[6].wait()


def table_body(bias_ref, out_ref):
    heads, pairs = out_ref.shape[:2]
    q = lax.broadcasted_iota(jnp.int32, (GRID_W, 2 * GRID_W), 0)
    lane = lax.broadcasted_iota(jnp.int32, (GRID_W, 2 * GRID_W), 1)
    k = lane & (GRID_W - 1)
    start = jnp.clip(q - WIN_COLS // 2, 0, GRID_W - WIN_COLS)
    is_open = (k >= start) & (k < start + WIN_COLS)
    low = lane < GRID_W
    width = 2 * GRID_W
    for h in range(heads):
        rolled = []
        for a in range(pairs + 1):
            row = jnp.broadcast_to(bias_ref[h, a : a + 1, :], (GRID_W, width))
            rolled.append(row)
        for a in range(pairs):
            first = pltpu.roll(rolled[a], (1 - WIN_COLS) % width, 1, stride=1, stride_axis=0)
            second = pltpu.roll(
                rolled[a + 1], (1 - WIN_COLS + GRID_W) % width, 1, stride=1, stride_axis=0
            )
            out_ref[h, a] = jnp.where(is_open, jnp.where(low, first, second), MASKED)


def head_norm(x, gain_row):
    cols = x.shape[1]
    r = lax.broadcasted_iota(jnp.int32, (cols, cols), 0) // HEAD_DIM
    c = lax.broadcasted_iota(jnp.int32, (cols, cols), 1) // HEAD_DIM
    same = jnp.where(r == c, 1.0 / HEAD_DIM, 0.0).astype(BF16)
    head_gain = jnp.concatenate([gain_row[...]] * (cols // HEAD_DIM), axis=1)
    square = x * x
    high = square.astype(BF16)
    rest = (square - high.astype(F32)).astype(BF16)
    mean = jnp.dot(high, same, preferred_element_type=F32) + jnp.dot(
        rest, same, preferred_element_type=F32
    )
    return x * lax.rsqrt(mean + EPS) * head_gain


def modulated(values, vec_ref, gain_ref, row):
    mult = gain_ref[...] * (1.0 + vec_ref[2 + row : 3 + row, :])
    shift = vec_ref[row : row + 1, :]
    mean = jnp.mean(values * values, axis=-1, keepdims=True)
    return (values * lax.rsqrt(mean + EPS) * mult + shift).astype(BF16)


def join_halves(mine_ref, passed_ref, out_ref):
    half = mine_ref.shape[1]
    core = lax.rem(lax.axis_index("tp"), 2)
    out_ref[:, pl.ds(pl.multiple_of(core * half, half), half)] = mine_ref[...]
    out_ref[:, pl.ds(pl.multiple_of((1 - core) * half, half), half)] = passed_ref[...]


def row_steps(count):
    step = 32 if count % 32 == 0 else count
    return [slice(at, at + step) for at in range(0, count, step)]


def project_body(codes, lat_ref, ctx_ref, mine_ref, passed_ref, part_ref, beside_ref, *refs):
    gain_ref, kg_ref, wk, wv = refs[:4]
    kv_ref, ckv_ref, lat_hid_ref, vec_ref = refs[4:8]
    hid_ref, ctx_two_ref = refs[8:]
    width = part_ref.shape[1]
    me = lax.axis_index("tp")
    for n, code in enumerate(codes):
        for ref, flip in ((part_ref, 0), (beside_ref, 1)):
            at = pl.multiple_of((me ^ code ^ flip) * width, width)
            vec_ref[:, pl.ds(at, width)] = ref[8 * n : 8 * n + 8, :]
    join_halves(mine_ref, passed_ref, ctx_two_ref)
    lat_count = lat_ref.shape[0]
    ctx_count = ctx_ref.shape[0]
    for here in row_steps(lat_count):
        lat_hid_ref[here, :] = modulated(lat_ref[here, :].astype(F32), vec_ref, gain_ref, 0)
    if ctx_count % 32:
        both = jnp.concatenate(
            [ctx_ref[...].astype(F32), ctx_two_ref[...].astype(F32)], axis=0
        )
        hid_ref[...] = modulated(both, vec_ref, gain_ref, 1)
    else:
        for n, ref in enumerate((ctx_ref, ctx_two_ref)):
            base = n * ctx_count
            for here in row_steps(ctx_count):
                hid_ref[base + here.start : base + here.stop, :] = modulated(
                    ref[here, :].astype(F32), vec_ref, gain_ref, 1
                )
    cols = wk.shape[1]
    for out, src in ((kv_ref, lat_hid_ref[...]), (ckv_ref, hid_ref[...])):
        out[:, :cols] = head_norm(
            jnp.dot(src, wk[...], preferred_element_type=F32), kg_ref
        ).astype(BF16)
        out[:, cols:] = jnp.dot(src, wv[...], preferred_element_type=F32).astype(BF16)


def near_body(
    mine_ref, passed_ref, vec_ref, gain_ref, kg_ref, wk, wv, own_hid_ref, wq, qg_ref,
    kv_ref, q_ref, lat_ref, hid_ref,
):
    queries = head_norm(
        jnp.dot(own_hid_ref[...], wq[...], preferred_element_type=F32), qg_ref
    ).astype(BF16)
    q_ref[...] = (queries.astype(F32) * HEAD_DIM ** (-0.5)).astype(BF16)
    join_halves(mine_ref, passed_ref, lat_ref)
    for here in row_steps(lat_ref.shape[0]):
        hid_ref[here, :] = modulated(lat_ref[here, :].astype(F32), vec_ref, gain_ref, 0)
    cols = wk.shape[1]
    step = lat_ref.shape[0] // 2
    for at in range(0, lat_ref.shape[0], step):
        hidden = hid_ref[at : at + step, :]
        kv_ref[at : at + step, :cols] = head_norm(
            jnp.dot(hidden, wk[...], preferred_element_type=F32), kg_ref
        ).astype(BF16)
        kv_ref[at : at + step, cols:] = jnp.dot(
            hidden, wv[...], preferred_element_type=F32
        ).astype(BF16)


OWN, NEAR, OTHER = range(3)


def attend_body(heads, lat_kinds, n_ctx, has_prev, is_last, q_ref, *refs):
    n_lat = len(lat_kinds)
    lat_refs, refs = refs[:n_lat], refs[n_lat:]
    ctx_refs, refs = refs[:n_ctx], refs[n_ctx:]
    if n_lat:
        table_ref, refs = refs[0], refs[1:]
    if has_prev:
        prev, refs = refs[:3], refs[3:]
    tokens, cols = q_ref.shape
    rows = tokens // GRID_W
    halo = WIN_ROWS // 2
    lane_head = lax.broadcasted_iota(jnp.int32, (1, cols), 1) // HEAD_DIM
    lane_row = lax.broadcasted_iota(jnp.int32, (1, 2 * GRID_W), 1) // GRID_W
    q_all = q_ref[...]
    parts = list(lat_refs) + list(ctx_refs)
    keys = [p[:, :cols] for p in parts]
    values = [p[:, cols:] for p in parts]
    sp_index = lax.axis_index("sp")
    first_row = sp_index * rows
    total_rows = rows * lax.axis_size("sp")
    starts = [
        jnp.clip(first_row + i - halo, 0, total_rows - WIN_ROWS) - first_row + halo
        for i in range(rows)
    ]
    is_odd = lax.rem(sp_index, 2)
    base_of = {
        OWN: halo,
        NEAR: (1 - is_odd) * (halo + rows),
        OTHER: is_odd * (halo + rows),
    }
    bases = [base_of[kind] for kind in lat_kinds]
    opens = {}
    for n in range(n_lat):
        for i in range(rows):
            for p in range(lat_refs[n].shape[0] // (2 * GRID_W)):
                row = lane_row + (bases[n] + 2 * p)
                start = starts[i]
                opens[n, i, p] = jnp.where(
                    (row >= start) & (row < start + WIN_ROWS), 0.0, MASKED
                )
    masks = [lane_head == h for h in range(heads)]
    all_scores = []
    for mine in masks:
        q_h = jnp.where(mine, q_all, jnp.zeros_like(q_all))
        all_scores.append([bt_dot(q_h, k) for k in keys])
    all_powers, tops, sums = [], None, None
    for h, scores in enumerate(all_scores):
        for n in range(n_lat):
            lines = []
            for i in range(rows):
                line = []
                for p in range(lat_refs[n].shape[0] // (2 * GRID_W)):
                    at = bases[n] + 2 * p - i + WIN_ROWS - 1 - halo
                    piece = scores[n][
                        i * GRID_W : (i + 1) * GRID_W, 2 * p * GRID_W : (2 * p + 2) * GRID_W
                    ]
                    line.append(piece + (table_ref[h, at] + opens[n, i, p]))
                lines.append(jnp.concatenate(line, axis=1))
            scores[n] = jnp.concatenate(lines, axis=0)
        top = functools.reduce(jnp.maximum, [jnp.max(s, axis=1, keepdims=True) for s in scores])
        powers = [jnp.exp(s - top) for s in scores]
        denom = functools.reduce(jnp.add, [jnp.sum(e, axis=1, keepdims=True) for e in powers])
        all_powers.append([e.astype(BF16) for e in powers])
        tops = jnp.broadcast_to(top, (tokens, cols)) if h == 0 else jnp.where(masks[h], top, tops)
        sums = jnp.broadcast_to(denom, (tokens, cols)) if h == 0 else jnp.where(masks[h], denom, sums)
    total = None
    for h, powers in enumerate(all_powers):
        acc = functools.reduce(
            jnp.add,
            [jnp.dot(e, v, preferred_element_type=F32) for e, v in zip(powers, values)],
        )
        total = acc if h == 0 else jnp.where(masks[h], acc, total)
    if has_prev:
        before = prev[0][...]
        both = jnp.maximum(before, tops)
        old = jnp.exp(before - both)
        new = jnp.exp(tops - both)
        tops = both
        sums = prev[1][...] * old + sums * new
        total = prev[2][...] * old + total * new
    if is_last:
        refs[0][...] = (total / sums).astype(BF16)
    else:
        for ref, value in zip(refs, (tops, sums, total)):
            ref[...] = value


def stash_body(*refs):
    count = len(refs) // 2
    sems = refs[-1]
    copies = [
        pltpu.make_async_copy(src, dst, sems.at[n])
        for n, (src, dst) in enumerate(zip(refs[:count], refs[count : 2 * count]))
    ]
    for copy in copies:
        copy.start()
    for copy in copies:
        copy.wait()


def first_body(count, has_prev, *refs):
    branch = None
    if has_prev:
        branch, refs = refs[0][...], refs[1:]
    att, weights, sum_ref = refs[:count], refs[count : 2 * count], refs[2 * count]
    for a, w in zip(att, weights):
        part = jnp.dot(a[...], w[...], preferred_element_type=F32).astype(BF16).astype(F32)
        branch = part if branch is None else branch + part
    sum_ref[...] = branch


def output_body(count, lat_ref, gate_ref, sum_ref, *refs):
    att = refs[:count]
    weights = refs[count : 2 * count]
    out_ref = refs[2 * count]
    branch = sum_ref[...]
    for a, w in zip(att, weights):
        branch = branch + jnp.dot(a[...], w[...], preferred_element_type=F32).astype(
            BF16
        ).astype(F32)
    out_ref[...] = (lat_ref[...].astype(F32) + gate_ref[4:5, :] * branch).astype(BF16)


def gather_pieces(x, axis, codes):
    pieces = [x]
    for code in codes:
        if len(pieces) > 2:
            pieces = [jnp.concatenate(pieces, axis=0)]
        pieces = pieces + [swap(p, axis, code) for p in pieces]
    return pieces


def gather_tp(x, codes):
    held = [(0, x)]
    for code in codes:
        held = held + [(had ^ code, swap(p, "tp", code)) for had, p in held]
    return held


def per_device(
    latent,
    context,
    condition,
    ctx_condition,
    shift_weight,
    scale_weight,
    gate_weight,
    norm_gain,
    query_weight,
    key_weight,
    value_weight,
    query_gain,
    key_gain,
    offset_bias,
    out_weight,
):
    sp_bits = bits_of("sp")
    tp_bits = bits_of("tp")[::-1]
    tokens, width = latent.shape
    cols = query_weight.shape[1]
    heads = cols // HEAD_DIM
    block_cols = shift_weight.shape[1]

    half = width // 2
    part, ctx_half, lat_half = call(
        partials_body,
        out_shape=(
            jax.ShapeDtypeStruct((8, block_cols), F32),
            jax.ShapeDtypeStruct((context.shape[0], half), BF16),
            jax.ShapeDtypeStruct((tokens, half), BF16),
        ),
        in_specs=raw(7),
        out_specs=tuple(vmem(3)),
        scratch_shapes=[pltpu.VMEM((2, condition.shape[0]), F32)]
        + [pltpu.VMEM(shift_weight.shape, BF16)] * 3
        + [pltpu.SemaphoreType.DMA((7,))],
        compiler_params=params(16),
        cost_estimate=pl.CostEstimate(flops=1 << 37, bytes_accessed=1 << 20, transcendentals=0),
    )(
        *[
            in_hbm(x)
            for x in (
                condition[None],
                ctx_condition[None],
                shift_weight,
                scale_weight,
                gate_weight,
                context,
                latent,
            )
        ]
    )
    raw_code = sp_bits[min(2, len(sp_bits) - 1)]
    ctx_mine = swap(ctx_half, "sp", raw_code)
    ctx_passed = swap(ctx_mine, "tp", 1)
    near_mine = swap(lat_half, "sp", 1)
    near_passed = swap(near_mine, "tp", 1)
    codes = [0]
    for code in tp_bits:
        if code > 1:
            part = jnp.concatenate([part, swap(part, "tp", code)], axis=0)
            codes = codes + [had ^ code for had in codes]
    for code in sp_bits:
        part = part + swap(part, "sp", code)
    beside = swap(part, "tp", 1)
    ow_blocks = gather_tp(out_weight, tp_bits)

    padded_bias = jnp.pad(offset_bias, ((0, 0), (0, 0), (0, LANES - offset_bias.shape[2])))
    tables = call(
        table_body,
        out_shape=jax.ShapeDtypeStruct((heads, 2 * WIN_ROWS - 2, GRID_W, 2 * GRID_W), F32),
        in_specs=vmem(1),
        out_specs=vmem(1)[0],
        compiler_params=params(16),
    )(padded_bias)

    ctx_count = 2 * context.shape[0]
    gain = norm_gain[None]
    kv, ctx_kv, hidden, vec = call(
        functools.partial(project_body, tuple(codes)),
        out_shape=(
            jax.ShapeDtypeStruct((tokens, 2 * cols), BF16),
            jax.ShapeDtypeStruct((ctx_count, 2 * cols), BF16),
            jax.ShapeDtypeStruct((tokens, width), BF16),
            jax.ShapeDtypeStruct((8, width), F32),
        ),
        in_specs=vmem(10),
        out_specs=vmem(4),
        scratch_shapes=[
            pltpu.VMEM((ctx_count, width), BF16),
            pltpu.VMEM(context.shape, BF16),
        ],
        compiler_params=params(20),
        cost_estimate=pl.CostEstimate(flops=1 << 37, bytes_accessed=1 << 20, transcendentals=0),
    )(
        latent,
        context,
        ctx_mine,
        ctx_passed,
        part,
        beside,
        gain,
        key_gain[None],
        key_weight,
        value_weight,
    )
    near_kv, queries = call(
        near_body,
        out_shape=(
            jax.ShapeDtypeStruct((tokens, 2 * cols), BF16),
            jax.ShapeDtypeStruct((tokens, cols), BF16),
        ),
        in_specs=vmem(10),
        out_specs=tuple(vmem(2)),
        scratch_shapes=[pltpu.VMEM((tokens, width), BF16)] * 2,
        compiler_params=params(20),
    )(
        near_mine,
        near_passed,
        vec,
        gain,
        key_gain[None],
        key_weight,
        value_weight,
        hidden,
        query_weight,
        query_gain[None],
    )
    sp_count = lax.axis_size("sp")
    other_pairs = [(i, i + 1) for i in range(1, sp_count - 1, 2)]
    other_pairs += [(j, i) for i, j in other_pairs]
    other_kv = lax.ppermute(kv, "sp", other_pairs)
    ctx_pieces = gather_pieces(ctx_kv, "sp", [code for code in sp_bits if code != raw_code])

    def attend(lat, lat_kinds, ctx, prev, is_last):
        shape = (tokens, cols)
        one = jax.ShapeDtypeStruct(shape, BF16)
        three = (jax.ShapeDtypeStruct(shape, F32),) * 3
        operands = [queries, *lat, *ctx] + ([tables] if lat else []) + list(prev)
        return call(
            functools.partial(
                attend_body, heads, lat_kinds, len(ctx), bool(prev), is_last
            ),
            out_shape=one if is_last else three,
            in_specs=vmem(len(operands)),
            out_specs=vmem(1)[0] if is_last else tuple(vmem(3)),
            compiler_params=params(24),
            cost_estimate=pl.CostEstimate(
                flops=1 << 37, bytes_accessed=1 << 20, transcendentals=0
            ),
        )(*operands)

    state = attend([kv, near_kv], (OWN, NEAR), ctx_pieces[:1], (), False)
    attended = attend([other_kv], (OTHER,), ctx_pieces[1:], state, True)

    att_blocks = gather_tp(attended, tp_bits)

    def stash(index):
        code, w = ow_blocks[index]
        (held,) = call(
            stash_body,
            out_shape=(jax.ShapeDtypeStruct((cols, width), BF16),),
            in_specs=raw(1),
            out_specs=tuple(vmem(1)),
            scratch_shapes=[pltpu.SemaphoreType.DMA((1,))],
            compiler_params=params(8),
        )(in_hbm(w))
        ow_blocks[index] = (code, held)

    for n in range(len(ow_blocks) // 2):
        stash(n)

    near = [n for n, (code, _) in enumerate(att_blocks) if code < 2]
    cross = [n for n, (code, _) in enumerate(att_blocks) if code > 1 and n < len(att_blocks) // 2]
    far = [n for n in range(len(att_blocks)) if n not in near + cross]
    tile = min(1024, width)
    att_spec = pl.BlockSpec((tokens, cols), lambda n: (0, 0))
    weight_spec = pl.BlockSpec((cols, tile), lambda n: (0, n))
    wide_spec = pl.BlockSpec((tokens, tile), lambda n: (0, n))

    def operands(which):
        return [att_blocks[n][1] for n in which] + [ow_blocks[n][1] for n in which]

    def specs(which):
        return [att_spec] * len(which) + [weight_spec] * len(which)

    partial_sum = call(
        functools.partial(first_body, len(near), False),
        out_shape=jax.ShapeDtypeStruct((tokens, width), F32),
        in_specs=vmem(2 * len(near)),
        out_specs=vmem(1)[0],
        compiler_params=params(24),
    )(*operands(near))
    partial_sum = call(
        functools.partial(first_body, len(cross), True),
        out_shape=jax.ShapeDtypeStruct((tokens, width), F32),
        in_specs=vmem(1 + 2 * len(cross)),
        out_specs=vmem(1)[0],
        compiler_params=params(24),
    )(partial_sum, *operands(cross))
    return call(
        functools.partial(output_body, len(far)),
        grid=(width // tile,),
        out_shape=jax.ShapeDtypeStruct((tokens, width), BF16),
        in_specs=[wide_spec, pl.BlockSpec((8, tile), lambda n: (0, n)), wide_spec]
        + specs(far),
        out_specs=wide_spec,
        compiler_params=params(24),
    )(latent, vec, partial_sum, *operands(far))


def solution(mesh):
    in_specs = (
        P("sp", None),
        P("sp", None),
        P("sp"),
        P("sp"),
        P("sp", "tp"),
        P("sp", "tp"),
        P("sp", "tp"),
        P(),
        P(None, "tp"),
        P(None, "tp"),
        P(None, "tp"),
        P(),
        P(),
        P("tp", None, None),
        P("tp", None),
    )
    out_specs = P("sp", None)
    return jax.shard_map(
        per_device, mesh=mesh, in_specs=in_specs, out_specs=out_specs, check_vma=False
    )
```

```python
import functools

import jax
import jax.numpy as jnp
from jax import lax
from jax.experimental import pallas as pl
from jax.experimental.pallas import tpu as pltpu
from jax.sharding import PartitionSpec as P


HEAD_DIM = 64
GRID_W = 64
WIN_ROWS = 8
WIN_COLS = 16
LANES = 128
EPS = 1e-06
MASKED = -1e30

F32 = jnp.float32
BF16 = jnp.bfloat16


def vmem(count):
    return [pl.BlockSpec(memory_space=pltpu.VMEM) for _ in range(count)]


def params(mib):
    return pltpu.CompilerParams(vmem_limit_bytes=mib << 20)


def swap(x, axis, code):
    return lax.ppermute(x, axis, [(i, i ^ code) for i in range(lax.axis_size(axis))])


def call(*args, **kwargs):
    def run(*operands):
        return pl.pallas_call(*args, **kwargs)(*operands)

    return run


def in_hbm(x):
    return pltpu.with_memory_space_constraint(x, pltpu.HBM)


def raw(count):
    return [pl.BlockSpec(memory_space=pltpu.HBM) for _ in range(count)]


def bits_of(axis):
    count = lax.axis_size(axis)
    return [1 << b for b in range(count.bit_length() - 1)]


def bt_dot(a, b):
    return lax.dot_general(a, b, (((1,), (1,)), ((), ())), preferred_element_type=F32)


def partials_body(
    cond_ref, ctx_cond_ref, shift_ref, scale_ref, gate_ref, ctx_ref, lat_ref,
    out_ref, ctx_half_ref, lat_half_ref, rows_ref, *scratch
):
    weights, sems = scratch[:3], scratch[3]
    half = ctx_half_ref.shape[1]
    at = pl.multiple_of(lax.rem(lax.axis_index("tp"), 2) * half, half)
    copies = [
        pltpu.make_async_copy(src, dst, sems.at[n])
        for n, (src, dst) in enumerate(
            (
                (cond_ref, rows_ref.at[0:1]),
                (ctx_cond_ref, rows_ref.at[1:2]),
                (shift_ref, weights[0]),
                (scale_ref, weights[1]),
                (gate_ref, weights[2]),
                (ctx_ref.at[:, pl.ds(at, half)], ctx_half_ref),
                (lat_ref.at[:, pl.ds(at, half)], lat_half_ref),
            )
        )
    ]
    for copy in copies:
        copy.start()
    copies[0].wait()
    copies[1].wait()
    rows = rows_ref[...]
    act = (rows / (1.0 + jnp.exp(-rows))).astype(BF16)
    for n in range(3):
        copies[2 + n].wait()
        out_ref[2 * n : 2 * n + 2, :] = jnp.dot(
            act, weights[n][...], preferred_element_type=F32
        )
    out_ref[6:8, :] = jnp.zeros((2, out_ref.shape[1]), F32)
    copies[5].wait()
    copies[6].wait()


def table_body(bias_ref, out_ref):
    heads, pairs = out_ref.shape[:2]
    q = lax.broadcasted_iota(jnp.int32, (GRID_W, 2 * GRID_W), 0)
    lane = lax.broadcasted_iota(jnp.int32, (GRID_W, 2 * GRID_W), 1)
    k = lane & (GRID_W - 1)
    start = jnp.clip(q - WIN_COLS // 2, 0, GRID_W - WIN_COLS)
    is_open = (k >= start) & (k < start + WIN_COLS)
    low = lane < GRID_W
    width = 2 * GRID_W
    for h in range(heads):
        rolled = []
        for a in range(pairs + 1):
            row = jnp.broadcast_to(bias_ref[h, a : a + 1, :], (GRID_W, width))
            rolled.append(row)
        for a in range(pairs):
            first = pltpu.roll(rolled[a], (1 - WIN_COLS) % width, 1, stride=1, stride_axis=0)
            second = pltpu.roll(
                rolled[a + 1], (1 - WIN_COLS + GRID_W) % width, 1, stride=1, stride_axis=0
            )
            out_ref[h, a] = jnp.where(is_open, jnp.where(low, first, second), MASKED)


def head_norm(x, gain_row):
    cols = x.shape[1]
    r = lax.broadcasted_iota(jnp.int32, (cols, cols), 0) // HEAD_DIM
    c = lax.broadcasted_iota(jnp.int32, (cols, cols), 1) // HEAD_DIM
    same = jnp.where(r == c, 1.0 / HEAD_DIM, 0.0).astype(BF16)
    head_gain = jnp.concatenate([gain_row[...]] * (cols // HEAD_DIM), axis=1)
    square = x * x
    high = square.astype(BF16)
    rest = (square - high.astype(F32)).astype(BF16)
    mean = jnp.dot(high, same, preferred_element_type=F32) + jnp.dot(
        rest, same, preferred_element_type=F32
    )
    return x * lax.rsqrt(mean + EPS) * head_gain


def modulated(values, vec_ref, gain_ref, row):
    mult = gain_ref[...] * (1.0 + vec_ref[2 + row : 3 + row, :])
    shift = vec_ref[row : row + 1, :]
    mean = jnp.mean(values * values, axis=-1, keepdims=True)
    return (values * lax.rsqrt(mean + EPS) * mult + shift).astype(BF16)


def join_halves(mine_ref, passed_ref, out_ref):
    half = mine_ref.shape[1]
    core = lax.rem(lax.axis_index("tp"), 2)
    out_ref[:, pl.ds(pl.multiple_of(core * half, half), half)] = mine_ref[...]
    out_ref[:, pl.ds(pl.multiple_of((1 - core) * half, half), half)] = passed_ref[...]


def row_steps(count):
    step = 32 if count % 32 == 0 else count
    return [slice(at, at + step) for at in range(0, count, step)]


def project_body(codes, lat_ref, ctx_ref, mine_ref, passed_ref, part_ref, beside_ref, *refs):
    gain_ref, kg_ref, wk, wv = refs[:4]
    kv_ref, ckv_ref, lat_hid_ref, vec_ref = refs[4:8]
    hid_ref, ctx_two_ref = refs[8:]
    width = part_ref.shape[1]
    me = lax.axis_index("tp")
    for n, code in enumerate(codes):
        for ref, flip in ((part_ref, 0), (beside_ref, 1)):
            at = pl.multiple_of((me ^ code ^ flip) * width, width)
            vec_ref[:, pl.ds(at, width)] = ref[8 * n : 8 * n + 8, :]
    join_halves(mine_ref, passed_ref, ctx_two_ref)
    lat_count = lat_ref.shape[0]
    ctx_count = ctx_ref.shape[0]
    for here in row_steps(lat_count):
        lat_hid_ref[here, :] = modulated(lat_ref[here, :].astype(F32), vec_ref, gain_ref, 0)
    if ctx_count % 32:
        both = jnp.concatenate(
            [ctx_ref[...].astype(F32), ctx_two_ref[...].astype(F32)], axis=0
        )
        hid_ref[...] = modulated(both, vec_ref, gain_ref, 1)
    else:
        for n, ref in enumerate((ctx_ref, ctx_two_ref)):
            base = n * ctx_count
            for here in row_steps(ctx_count):
                hid_ref[base + here.start : base + here.stop, :] = modulated(
                    ref[here, :].astype(F32), vec_ref, gain_ref, 1
                )
    cols = wk.shape[1]
    for out, src in ((kv_ref, lat_hid_ref[...]), (ckv_ref, hid_ref[...])):
        out[:, :cols] = head_norm(
            jnp.dot(src, wk[...], preferred_element_type=F32), kg_ref
        ).astype(BF16)
        out[:, cols:] = jnp.dot(src, wv[...], preferred_element_type=F32).astype(BF16)


def near_body(
    mine_ref, passed_ref, vec_ref, gain_ref, kg_ref, wk, wv, own_hid_ref, wq, qg_ref,
    kv_ref, q_ref, lat_ref, hid_ref,
):
    queries = head_norm(
        jnp.dot(own_hid_ref[...], wq[...], preferred_element_type=F32), qg_ref
    ).astype(BF16)
    q_ref[...] = (queries.astype(F32) * HEAD_DIM ** (-0.5)).astype(BF16)
    join_halves(mine_ref, passed_ref, lat_ref)
    for here in row_steps(lat_ref.shape[0]):
        hid_ref[here, :] = modulated(lat_ref[here, :].astype(F32), vec_ref, gain_ref, 0)
    cols = wk.shape[1]
    step = lat_ref.shape[0] // 2
    for at in range(0, lat_ref.shape[0], step):
        hidden = hid_ref[at : at + step, :]
        kv_ref[at : at + step, :cols] = head_norm(
            jnp.dot(hidden, wk[...], preferred_element_type=F32), kg_ref
        ).astype(BF16)
        kv_ref[at : at + step, cols:] = jnp.dot(
            hidden, wv[...], preferred_element_type=F32
        ).astype(BF16)


OWN, NEAR, OTHER = range(3)


def attend_body(heads, lat_kinds, n_ctx, has_prev, is_last, q_ref, *refs):
    n_lat = len(lat_kinds)
    lat_refs, refs = refs[:n_lat], refs[n_lat:]
    ctx_refs, refs = refs[:n_ctx], refs[n_ctx:]
    if n_lat:
        table_ref, refs = refs[0], refs[1:]
    if has_prev:
        prev, refs = refs[:3], refs[3:]
    tokens, cols = q_ref.shape
    rows = tokens // GRID_W
    halo = WIN_ROWS // 2
    lane_head = lax.broadcasted_iota(jnp.int32, (1, cols), 1) // HEAD_DIM
    lane_row = lax.broadcasted_iota(jnp.int32, (1, 2 * GRID_W), 1) // GRID_W
    q_all = q_ref[...]
    parts = list(lat_refs) + list(ctx_refs)
    keys = [p[:, :cols] for p in parts]
    values = [p[:, cols:] for p in parts]
    sp_index = lax.axis_index("sp")
    first_row = sp_index * rows
    total_rows = rows * lax.axis_size("sp")
    starts = [
        jnp.clip(first_row + i - halo, 0, total_rows - WIN_ROWS) - first_row + halo
        for i in range(rows)
    ]
    is_odd = lax.rem(sp_index, 2)
    base_of = {
        OWN: halo,
        NEAR: (1 - is_odd) * (halo + rows),
        OTHER: is_odd * (halo + rows),
    }
    bases = [base_of[kind] for kind in lat_kinds]
    opens = {}
    for n in range(n_lat):
        for i in range(rows):
            for p in range(lat_refs[n].shape[0] // (2 * GRID_W)):
                row = lane_row + (bases[n] + 2 * p)
                start = starts[i]
                opens[n, i, p] = jnp.where(
                    (row >= start) & (row < start + WIN_ROWS), 0.0, MASKED
                )
    masks = [lane_head == h for h in range(heads)]
    all_scores = []
    for mine in masks:
        q_h = jnp.where(mine, q_all, jnp.zeros_like(q_all))
        all_scores.append([bt_dot(q_h, k) for k in keys])
    all_powers, tops, sums = [], None, None
    for h, scores in enumerate(all_scores):
        for n in range(n_lat):
            lines = []
            for i in range(rows):
                line = []
                for p in range(lat_refs[n].shape[0] // (2 * GRID_W)):
                    at = bases[n] + 2 * p - i + WIN_ROWS - 1 - halo
                    piece = scores[n][
                        i * GRID_W : (i + 1) * GRID_W, 2 * p * GRID_W : (2 * p + 2) * GRID_W
                    ]
                    line.append(piece + (table_ref[h, at] + opens[n, i, p]))
                lines.append(jnp.concatenate(line, axis=1))
            scores[n] = jnp.concatenate(lines, axis=0)
        top = functools.reduce(jnp.maximum, [jnp.max(s, axis=1, keepdims=True) for s in scores])
        powers = [jnp.exp(s - top) for s in scores]
        denom = functools.reduce(jnp.add, [jnp.sum(e, axis=1, keepdims=True) for e in powers])
        all_powers.append([e.astype(BF16) for e in powers])
        tops = jnp.broadcast_to(top, (tokens, cols)) if h == 0 else jnp.where(masks[h], top, tops)
        sums = jnp.broadcast_to(denom, (tokens, cols)) if h == 0 else jnp.where(masks[h], denom, sums)
    total = None
    for h, powers in enumerate(all_powers):
        acc = functools.reduce(
            jnp.add,
            [jnp.dot(e, v, preferred_element_type=F32) for e, v in zip(powers, values)],
        )
        total = acc if h == 0 else jnp.where(masks[h], acc, total)
    if has_prev:
        before = prev[0][...]
        both = jnp.maximum(before, tops)
        old = jnp.exp(before - both)
        new = jnp.exp(tops - both)
        tops = both
        sums = prev[1][...] * old + sums * new
        total = prev[2][...] * old + total * new
    if is_last:
        refs[0][...] = (total / sums).astype(BF16)
    else:
        for ref, value in zip(refs, (tops, sums, total)):
            ref[...] = value


def stash_body(*refs):
    count = len(refs) // 2
    sems = refs[-1]
    copies = [
        pltpu.make_async_copy(src, dst, sems.at[n])
        for n, (src, dst) in enumerate(zip(refs[:count], refs[count : 2 * count]))
    ]
    for copy in copies:
        copy.start()
    for copy in copies:
        copy.wait()


def first_body(count, has_prev, *refs):
    branch = None
    if has_prev:
        branch, refs = refs[0][...], refs[1:]
    att, weights, sum_ref = refs[:count], refs[count : 2 * count], refs[2 * count]
    for a, w in zip(att, weights):
        part = jnp.dot(a[...], w[...], preferred_element_type=F32).astype(BF16).astype(F32)
        branch = part if branch is None else branch + part
    sum_ref[...] = branch


def output_body(count, lat_ref, gate_ref, sum_ref, *refs):
    att = refs[:count]
    weights = refs[count : 2 * count]
    out_ref = refs[2 * count]
    branch = sum_ref[...]
    for a, w in zip(att, weights):
        branch = branch + jnp.dot(a[...], w[...], preferred_element_type=F32).astype(
            BF16
        ).astype(F32)
    out_ref[...] = (lat_ref[...].astype(F32) + gate_ref[4:5, :] * branch).astype(BF16)


def gather_pieces(x, axis, codes):
    pieces = [x]
    for code in codes:
        if len(pieces) > 2:
            pieces = [jnp.concatenate(pieces, axis=0)]
        pieces = pieces + [swap(p, axis, code) for p in pieces]
    return pieces


def gather_tp(x, codes):
    held = [(0, x)]
    for code in codes:
        held = held + [(had ^ code, swap(p, "tp", code)) for had, p in held]
    return held


def per_device(
    latent,
    context,
    condition,
    ctx_condition,
    shift_weight,
    scale_weight,
    gate_weight,
    norm_gain,
    query_weight,
    key_weight,
    value_weight,
    query_gain,
    key_gain,
    offset_bias,
    out_weight,
):
    sp_bits = bits_of("sp")
    tp_bits = bits_of("tp")[::-1]
    tokens, width = latent.shape
    cols = query_weight.shape[1]
    heads = cols // HEAD_DIM
    block_cols = shift_weight.shape[1]

    half = width // 2
    part, ctx_half, lat_half = call(
        partials_body,
        out_shape=(
            jax.ShapeDtypeStruct((8, block_cols), F32),
            jax.ShapeDtypeStruct((context.shape[0], half), BF16),
            jax.ShapeDtypeStruct((tokens, half), BF16),
        ),
        in_specs=raw(7),
        out_specs=tuple(vmem(3)),
        scratch_shapes=[pltpu.VMEM((2, condition.shape[0]), F32)]
        + [pltpu.VMEM(shift_weight.shape, BF16)] * 3
        + [pltpu.SemaphoreType.DMA((7,))],
        compiler_params=params(16),
        cost_estimate=pl.CostEstimate(flops=1 << 37, bytes_accessed=1 << 20, transcendentals=0),
    )(
        *[
            in_hbm(x)
            for x in (
                condition[None],
                ctx_condition[None],
                shift_weight,
                scale_weight,
                gate_weight,
                context,
                latent,
            )
        ]
    )
    raw_code = sp_bits[min(2, len(sp_bits) - 1)]
    ctx_mine = swap(ctx_half, "sp", raw_code)
    ctx_passed = swap(ctx_mine, "tp", 1)
    near_mine = swap(lat_half, "sp", 1)
    near_passed = swap(near_mine, "tp", 1)
    codes = [0]
    for code in tp_bits:
        if code > 1:
            part = jnp.concatenate([part, swap(part, "tp", code)], axis=0)
            codes = codes + [had ^ code for had in codes]
    for code in sp_bits:
        part = part + swap(part, "sp", code)
    beside = swap(part, "tp", 1)
    ow_blocks = gather_tp(out_weight, tp_bits)

    padded_bias = jnp.pad(offset_bias, ((0, 0), (0, 0), (0, LANES - offset_bias.shape[2])))
    tables = call(
        table_body,
        out_shape=jax.ShapeDtypeStruct((heads, 2 * WIN_ROWS - 2, GRID_W, 2 * GRID_W), F32),
        in_specs=vmem(1),
        out_specs=vmem(1)[0],
        compiler_params=params(16),
    )(padded_bias)

    ctx_count = 2 * context.shape[0]
    gain = norm_gain[None]
    kv, ctx_kv, hidden, vec = call(
        functools.partial(project_body, tuple(codes)),
        out_shape=(
            jax.ShapeDtypeStruct((tokens, 2 * cols), BF16),
            jax.ShapeDtypeStruct((ctx_count, 2 * cols), BF16),
            jax.ShapeDtypeStruct((tokens, width), BF16),
            jax.ShapeDtypeStruct((8, width), F32),
        ),
        in_specs=vmem(10),
        out_specs=vmem(4),
        scratch_shapes=[
            pltpu.VMEM((ctx_count, width), BF16),
            pltpu.VMEM(context.shape, BF16),
        ],
        compiler_params=params(20),
        cost_estimate=pl.CostEstimate(flops=1 << 37, bytes_accessed=1 << 20, transcendentals=0),
    )(
        latent,
        context,
        ctx_mine,
        ctx_passed,
        part,
        beside,
        gain,
        key_gain[None],
        key_weight,
        value_weight,
    )
    near_kv, queries = call(
        near_body,
        out_shape=(
            jax.ShapeDtypeStruct((tokens, 2 * cols), BF16),
            jax.ShapeDtypeStruct((tokens, cols), BF16),
        ),
        in_specs=vmem(10),
        out_specs=tuple(vmem(2)),
        scratch_shapes=[pltpu.VMEM((tokens, width), BF16)] * 2,
        compiler_params=params(20),
    )(
        near_mine,
        near_passed,
        vec,
        gain,
        key_gain[None],
        key_weight,
        value_weight,
        hidden,
        query_weight,
        query_gain[None],
    )
    sp_count = lax.axis_size("sp")
    other_pairs = [(i, i + 1) for i in range(1, sp_count - 1, 2)]
    other_pairs += [(j, i) for i, j in other_pairs]
    other_kv = lax.ppermute(kv, "sp", other_pairs)
    rest = [code for code in sp_bits if code != raw_code]
    ctx_pieces = [ctx_kv]
    for code in (rest[0], rest[1], rest[0] | rest[1]):
        ctx_pieces.append(swap(ctx_kv, "sp", code))
    if rest[2:]:
        whole = jnp.concatenate(ctx_pieces, axis=0)
        ctx_pieces = gather_pieces(whole, "sp", rest[2:])

    def attend(lat, lat_kinds, ctx, prev, is_last):
        shape = (tokens, cols)
        one = jax.ShapeDtypeStruct(shape, BF16)
        three = (jax.ShapeDtypeStruct(shape, F32),) * 3
        operands = [queries, *lat, *ctx] + ([tables] if lat else []) + list(prev)
        return call(
            functools.partial(
                attend_body, heads, lat_kinds, len(ctx), bool(prev), is_last
            ),
            out_shape=one if is_last else three,
            in_specs=vmem(len(operands)),
            out_specs=vmem(1)[0] if is_last else tuple(vmem(3)),
            compiler_params=params(24),
            cost_estimate=pl.CostEstimate(
                flops=1 << 37, bytes_accessed=1 << 20, transcendentals=0
            ),
        )(*operands)

    state = attend([kv, near_kv], (OWN, NEAR), ctx_pieces[:1], (), False)
    attended = attend([other_kv], (OTHER,), ctx_pieces[1:], state, True)

    att_blocks = gather_tp(attended, tp_bits)

    def stash(index):
        code, w = ow_blocks[index]
        (held,) = call(
            stash_body,
            out_shape=(jax.ShapeDtypeStruct((cols, width), BF16),),
            in_specs=raw(1),
            out_specs=tuple(vmem(1)),
            scratch_shapes=[pltpu.SemaphoreType.DMA((1,))],
            compiler_params=params(8),
        )(in_hbm(w))
        ow_blocks[index] = (code, held)

    for n in range(len(ow_blocks) // 2):
        stash(n)

    near = [n for n, (code, _) in enumerate(att_blocks) if code < 2]
    cross = [n for n, (code, _) in enumerate(att_blocks) if code > 1 and n < len(att_blocks) // 2]
    far = [n for n in range(len(att_blocks)) if n not in near + cross]
    tile = min(1024, width)
    att_spec = pl.BlockSpec((tokens, cols), lambda n: (0, 0))
    weight_spec = pl.BlockSpec((cols, tile), lambda n: (0, n))
    wide_spec = pl.BlockSpec((tokens, tile), lambda n: (0, n))

    def operands(which):
        return [att_blocks[n][1] for n in which] + [ow_blocks[n][1] for n in which]

    def specs(which):
        return [att_spec] * len(which) + [weight_spec] * len(which)

    partial_sum = call(
        functools.partial(first_body, len(near), False),
        out_shape=jax.ShapeDtypeStruct((tokens, width), F32),
        in_specs=vmem(2 * len(near)),
        out_specs=vmem(1)[0],
        compiler_params=params(24),
    )(*operands(near))
    partial_sum = call(
        functools.partial(first_body, len(cross), True),
        out_shape=jax.ShapeDtypeStruct((tokens, width), F32),
        in_specs=vmem(1 + 2 * len(cross)),
        out_specs=vmem(1)[0],
        compiler_params=params(24),
    )(partial_sum, *operands(cross))
    return call(
        functools.partial(output_body, len(far)),
        grid=(width // tile,),
        out_shape=jax.ShapeDtypeStruct((tokens, width), BF16),
        in_specs=[wide_spec, pl.BlockSpec((8, tile), lambda n: (0, n)), wide_spec]
        + specs(far),
        out_specs=wide_spec,
        compiler_params=params(24),
    )(latent, vec, partial_sum, *operands(far))


def solution(mesh):
    in_specs = (
        P("sp", None),
        P("sp", None),
        P("sp"),
        P("sp"),
        P("sp", "tp"),
        P("sp", "tp"),
        P("sp", "tp"),
        P(),
        P(None, "tp"),
        P(None, "tp"),
        P(None, "tp"),
        P(),
        P(),
        P("tp", None, None),
        P("tp", None),
    )
    out_specs = P("sp", None)
    return jax.shard_map(
        per_device, mesh=mesh, in_specs=in_specs, out_specs=out_specs, check_vma=False
    )
```
